128 devices in a mesh: sp: 16 (over z, x), tp: 8 (over y, core).
Axes of the slice: x: 4, y: 4, z: 4, core: 2. Of those that a mesh axis runs over, the one named last changes fastest.
Arguments:
- queries: bfloat16 [16384, 1024], P('sp', 'tp'), may hold values from -75 to 75
- key_rows: bfloat16 [16384, 1024], P('sp', 'tp'), may hold values from -4 to 4
- value_rows: bfloat16 [16384, 1024], P('sp', 'tp'), may hold values from -6 to 6
- cum_gate: float32 [16, 16384], P('tp'), may hold values from -2342 to 0, as said below
- residual: bfloat16 [16384, 2048], P(('sp', 'tp')), may hold values from -6 to 6
- out_weight: bfloat16 [1024, 2048], replicated, may hold values from -0.1875 to 0.1875
- gain_mix: float32 [2048], replicated, may hold values from 0.1 to 1.9
- gain_pre: float32 [2048], replicated, may hold values from 0.1 to 1.9
- gain_post: float32 [2048], replicated, may hold values from 0.1 to 1.9
- route_ids: int32 [16384, 2], P(('sp', 'tp')), may hold values from 0 to 127, all different within a row; in each aligned block of 128 rows (0 to 127, 128 to 255, ...) at most 3 rows name the same one
- route_weight: float32 [16384, 2], P(('sp', 'tp')), may hold values from 0.2 to 1
- w_gate: bfloat16 [128, 2048, 512], P(('sp', 'tp')), may hold values from -0.125 to 0.125
- w_up: bfloat16 [128, 2048, 512], P(('sp', 'tp')), may hold values from -0.125 to 0.125
- w_down: bfloat16 [128, 512, 2048], P(('sp', 'tp')), may hold values from -0.25 to 0.25
Outputs:
- layer_out: bfloat16 [16384, 2048], P(('sp', 'tp'))
The draws below stay inside these ranges and needn't reach their ends.
Inputs may be any that keep to these rules, and one draw needn't show every extreme that they name: `route_ids`: each row names 2 different experts; in the rows of one device no expert is named more than 3 times, a bound that some block reaches. `cum_gate`: along the positions each head's values never rise.
All inputs are finite; a program needn't handle non-finite values.
Results may differ from the reference program's by a relative error of at most 0.018.
Values may be sent and summed in bfloat16 or wider, within the bound.
A program may use at most 64 MiB of HBM per device.

```python
import math
import jax
import jax.numpy as jnp
import numpy as np
from jax import lax

D = 2048
ATTENTION_HEADS = 16
HEAD_DIM = 64
FF = 512
TOP = 2
TOK_DEV = 1024
TOKEN_COUNT = 16384
ROWS = 128
EXPERTS = 128
CAP = 3
N_SP = 16
N_TP = 8


def draw_queries(key, part):
    sample = jax.random.normal(jax.random.fold_in(key, 1), (TOKEN_COUNT, ATTENTION_HEADS * HEAD_DIM), jnp.float32)
    return jnp.clip(sample, -4.0, 4.0).astype(jnp.bfloat16)


def draw_key_rows(key, part):
    sample = jax.random.normal(jax.random.fold_in(key, 2), (TOKEN_COUNT, ATTENTION_HEADS * HEAD_DIM), jnp.float32)
    return jnp.clip(sample, -4.0, 4.0).astype(jnp.bfloat16)


def draw_cum_gate(key, part):
    key_o, key_s, key_f, key_r, key_b, random_key_position, random_key_log = jax.random.split(jax.random.fold_in(key, 5), 7)
    shuffle = jax.random.permutation(key_o, ATTENTION_HEADS)
    slow_head = shuffle < ATTENTION_HEADS // 2
    slow_total = jax.random.uniform(key_s, (ATTENTION_HEADS,), jnp.float32, 0.4, 1.0)
    fast_rate = jnp.exp(jax.random.uniform(key_f, (ATTENTION_HEADS,), jnp.float32, -4.6, -3.4))
    step_rate = jnp.where(slow_head, slow_total / TOKEN_COUNT, fast_rate)
    blocks = TOKEN_COUNT // TOK_DEV
    roughness = jnp.exp(jax.random.uniform(key_r, (ATTENTION_HEADS, blocks, TOK_DEV), jnp.float32, -0.7, 0.7))
    block_factor = jnp.exp(jax.random.uniform(key_b, (ATTENTION_HEADS, blocks, 1), jnp.float32, -0.7, 0.7))
    logarithm_steps = step_rate[:, None] * (roughness * block_factor).reshape(ATTENTION_HEADS, TOKEN_COUNT)
    spike_position = jax.random.randint(random_key_position, (ATTENTION_HEADS, 2), 0, TOKEN_COUNT)
    spike_decay = -jnp.log(1.0 - jax.random.uniform(random_key_log, (ATTENTION_HEADS, 2), jnp.float32, 0.2, 0.45))
    index_of_head = jnp.broadcast_to(lax.iota(jnp.int32, ATTENTION_HEADS)[:, None], (ATTENTION_HEADS, 2))
    logarithm_steps = logarithm_steps.at[index_of_head, spike_position].add(spike_decay)
    return -jnp.cumsum(logarithm_steps, axis=1)


def steps_of(own_key, extent, cuts, least, high):
    def one(position, parts):
        draws = jax.random.uniform(jax.random.fold_in(jax.random.fold_in(own_key, 6), position), (parts,), jnp.float32, least / len(cuts), high / len(cuts))
        return jnp.repeat(jnp.exp(draws), extent[position] // parts).reshape((-1,) + (1,) * (len(extent) - position - 1))

    level = one(*cuts[0])
    for cut in cuts[1:]:
        level = level * one(*cut)
    return level


def shared_out(own_key, own, number, rows, number_of, top, bound, skew):
    ranking = jax.random.permutation(own_key, number_of)
    heavy_load, ordinary = shares(number_of, rows * top, bound, skew, True), shares(number_of, rows * top, bound, skew, False)
    places = jnp.arange(number_of)

    def named(lengths, offset_by):
        used = int((lengths > 0).sum())
        fixed = max(1, used // 4)
        passed = fixed + (places - fixed + offset_by * (used - fixed)) % max(1, number_of - fixed)
        return jnp.zeros((number_of,), jnp.int32).at[ranking[jnp.where(places < fixed, places, passed)]].set(jnp.asarray(lengths, jnp.int32))

    lengths = jnp.where(number % 4 == 0, named(heavy_load, number // 4), named(ordinary, number - number // 4 - 1))
    mixed = jax.random.permutation(jax.random.fold_in(own, 3), number_of)
    source_of, taker = mixed[0:number_of // 2 * 2:2], mixed[1:number_of // 2 * 2:2]
    slack = jnp.minimum(lengths[source_of] - 1, bound - lengths[taker]) // 2
    slack = jnp.where((source_of == ranking[0]) | (taker == ranking[0]) | (lengths[taker] == 0), 0, jnp.maximum(slack, 0))
    passed = jax.random.randint(jax.random.fold_in(own, 4), (number_of // 2,), 0, 1 << 20) % (slack + 1)
    lengths = lengths.at[source_of].add(-passed).at[taker].add(passed)
    labels = jnp.searchsorted(jnp.cumsum(lengths), jnp.arange(rows * top), side="right").astype(jnp.int32)
    grid = labels.reshape(top, rows).T
    grid = grid[jax.random.permutation(jax.random.fold_in(own, 1), rows)]
    offset_by = jax.random.randint(jax.random.fold_in(own, 2), (rows, 1), 0, top)
    return jnp.take_along_axis(grid, (jnp.arange(top)[None, :] + offset_by) % top, axis=1)


def shares(count, total, reach, skew, full):
    portions = [(1 << 20) // math.isqrt(rank ** skew) + 1 for rank in range(1, count + 1)]
    largest = reach if full else min(reach, max(-(-total // count), total * portions[0] // sum(portions)))
    least = 1 if total - largest >= count - 1 else 0
    holding, spare = [largest] + [least] * (count - 1), total - largest - least * (count - 1)
    while spare > 0:
        free = [i for i in range(1, count) if holding[i] < largest] or [i for i in range(1, count) if holding[i] < reach]
        pool, remaining = sum([portions[i] for i in free]), spare
        for i in free:
            more = min(reach - holding[i], max(1, remaining * portions[i] // pool), spare)
            holding[i] = holding[i] + more
            spare = spare - more
    return np.array(holding)


def scatter_about(own_key, dims, deviation, reach, shards=(), kind=jnp.bfloat16):
    values = jax.random.normal(own_key, dims, jnp.float32) * deviation
    if len(shards) > 0:
        values = steps_of(own_key, dims, shards, -0.22, 0.18) * values
    return jnp.clip(values, min=-reach, max=reach).astype(kind)


def setup_inputs(seed: int = 0) -> dict:
    keys = jax.random.split(jax.random.key(seed), 15)
    queries = draw_queries(jax.random.fold_in(keys[14], 71), 0)
    key_rows = draw_key_rows(jax.random.fold_in(keys[14], 71), 0)
    value_rows = scatter_about(keys[2], (TOKEN_COUNT, ATTENTION_HEADS * HEAD_DIM), 1.0, 6.0, ((0, 16), (1, 8)))
    cum_gate = draw_cum_gate(jax.random.fold_in(keys[14], 71), 0)
    residual = scatter_about(keys[4], (TOKEN_COUNT, D), 1.0, 6.0, ((0, 128),))
    out_weight = scatter_about(keys[5], (ATTENTION_HEADS * HEAD_DIM, D), (ATTENTION_HEADS * HEAD_DIM) ** -0.5, 0.1875)
    gain_mix = jnp.clip(1.0 + 0.18 * jax.random.normal(keys[6], (D,), jnp.float32), 0.1, 1.9)
    gain_pre = jnp.clip(1.0 + 0.18 * jax.random.normal(keys[7], (D,), jnp.float32), 0.1, 1.9)
    gain_post = jnp.clip(1.0 + 0.18 * jax.random.normal(keys[8], (D,), jnp.float32), 0.1, 1.9)
    route_ids_keys = jax.random.split(jax.random.fold_in(keys[9], 1), TOKEN_COUNT // ROWS)
    route_ids_turns = jax.random.permutation(jax.random.fold_in(keys[9], 3), TOKEN_COUNT // ROWS)
    route_ids = jax.vmap(lambda own, number: shared_out(jax.random.fold_in(keys[9], 2), own, number, ROWS, EXPERTS, TOP, CAP, 1))(route_ids_keys, route_ids_turns).reshape((TOKEN_COUNT, TOP))
    route_weight = jnp.clip(jnp.exp(math.log(1.0) - 1.609438 * jax.random.uniform(keys[10], (TOKEN_COUNT, TOP), jnp.float32) ** steps_of(keys[10], (TOKEN_COUNT, TOP), ((0, 128),), -0.2, 0.2)), 0.2, 1.0)
    w_gate = scatter_about(keys[11], (EXPERTS, D, FF), D ** -0.5, 0.125, ((0, 128),))
    w_up = scatter_about(keys[12], (EXPERTS, D, FF), D ** -0.5, 0.125, ((0, 128),))
    w_down = scatter_about(keys[13], (EXPERTS, FF, D), FF ** -0.5, 0.25, ((0, 128),))
    return {"queries": queries, "key_rows": key_rows, "value_rows": value_rows, "cum_gate": cum_gate, "residual": residual, "out_weight": out_weight, "gain_mix": gain_mix, "gain_pre": gain_pre, "gain_post": gain_post, "route_ids": route_ids, "route_weight": route_weight, "w_gate": w_gate, "w_up": w_up, "w_down": w_down}


NORM_EPS = 1e-06
MASKED = -1e+30

def rms_scale(rows, gain):
    mean_sq = lax.optimization_barrier(jnp.mean(rows * rows, axis=-1, keepdims=True))
    return rows * lax.rsqrt(mean_sq + NORM_EPS) * gain

def attend(running, queries, gate_q, q_start, key_part, value_part, gate_k, k_start):
    row_peak, row_total, weighted = running
    scores = jnp.einsum('qhd,khd->hqk', queries.astype(jnp.float32), key_part.astype(jnp.float32)) * HEAD_DIM ** (-0.5)
    scores = scores + gate_q[:, :, None] - gate_k[:, None, :]
    query_pos = q_start + lax.iota(jnp.int32, queries.shape[0])
    key_pos = k_start + lax.iota(jnp.int32, key_part.shape[0])
    allowed = (key_pos[None, :] <= query_pos[:, None])[None]
    scores = jnp.where(allowed, scores, MASKED)
    new_peak = jnp.maximum(row_peak, lax.optimization_barrier(jnp.max(scores, axis=-1)))
    unnorm = jnp.where(allowed, jnp.exp(scores - new_peak[..., None]), 0.0)
    rescale = jnp.exp(row_peak - new_peak)
    row_total = row_total * rescale + lax.optimization_barrier(jnp.sum(unnorm, axis=-1))
    probs = lax.optimization_barrier(unnorm.astype(jnp.bfloat16)).astype(jnp.float32)
    weighted = weighted * rescale.T[:, :, None] + jnp.einsum('hqk,khd->qhd', probs, value_part.astype(jnp.float32))
    return (new_peak, row_total, weighted)

def attention(queries, key_rows, value_rows, cum_gate):
    query_heads = queries.reshape(TOKEN_COUNT, ATTENTION_HEADS, HEAD_DIM)
    key_heads = key_rows.reshape(TOKEN_COUNT, ATTENTION_HEADS, HEAD_DIM)
    value_heads = value_rows.reshape(TOKEN_COUNT, ATTENTION_HEADS, HEAD_DIM)

    def one_block(block_index):
        q_start = block_index * TOK_DEV
        query_block = lax.dynamic_slice_in_dim(query_heads, q_start, TOK_DEV, 0)
        gate_q = lax.dynamic_slice_in_dim(cum_gate, q_start, TOK_DEV, 1)
        initial = (jnp.full((ATTENTION_HEADS, TOK_DEV), MASKED, jnp.float32), jnp.zeros((ATTENTION_HEADS, TOK_DEV), jnp.float32), jnp.zeros((TOK_DEV, ATTENTION_HEADS, HEAD_DIM), jnp.float32))

        def key_block(other, running):
            k_start = (other * TOK_DEV).astype(jnp.int32)
            return attend(running, query_block, gate_q, q_start, lax.dynamic_slice_in_dim(key_heads, k_start, TOK_DEV, 0), lax.dynamic_slice_in_dim(value_heads, k_start, TOK_DEV, 0), lax.dynamic_slice_in_dim(cum_gate, k_start, TOK_DEV, 1), k_start)
        row_peak, row_total, weighted = lax.fori_loop(jnp.int32(0), block_index + 1, key_block, initial)
        return (weighted / row_total.T[:, :, None]).astype(jnp.bfloat16)
    blocks = lax.map(one_block, jnp.arange(N_SP, dtype=jnp.int32))
    return blocks.reshape(TOKEN_COUNT, ATTENTION_HEADS * HEAD_DIM)

def route_experts(normed, route_ids, route_weight, w_gate, w_up, w_down):
    sources = N_SP * N_TP
    flat_ids = route_ids.reshape(sources, ROWS * TOP)
    onehot = (flat_ids[:, :, None] == jnp.arange(EXPERTS, dtype=jnp.int32)[None, None, :]).astype(jnp.int32)
    slot_rank = (lax.optimization_barrier(jnp.sum(jnp.cumsum(onehot, axis=1) * onehot, axis=2)) - 1).astype(jnp.int32)
    slot_index = flat_ids * (sources * CAP) + jnp.arange(sources, dtype=jnp.int32)[:, None] * CAP + slot_rank
    slot_index = slot_index.reshape(-1).astype(jnp.int32)
    token_index = jnp.arange(TOKEN_COUNT * TOP, dtype=jnp.int32) // TOP
    slot_count = EXPERTS * sources * CAP
    source_row = jnp.zeros((slot_count,), jnp.int32).at[slot_index].set(token_index)
    slot_weight = jnp.zeros((slot_count,), jnp.float32).at[slot_index].set(route_weight.reshape(-1))

    def one_expert(summed, expert):
        offset = (expert * sources * CAP).astype(jnp.int32)
        picked_rows = lax.dynamic_slice_in_dim(source_row, offset, sources * CAP)
        weights = lax.dynamic_slice_in_dim(slot_weight, offset, sources * CAP)
        routed = normed[picked_rows]
        gate_act = jnp.dot(routed, w_gate[expert], preferred_element_type=jnp.float32)
        up_act = jnp.dot(routed, w_up[expert], preferred_element_type=jnp.float32)
        hidden = (jax.nn.silu(gate_act) * up_act).astype(jnp.bfloat16)
        result = jnp.dot(hidden, w_down[expert], preferred_element_type=jnp.float32).astype(jnp.bfloat16)
        summed = summed.at[picked_rows].add(weights[:, None] * result.astype(jnp.float32))
        return (summed, None)
    summed, _ = lax.scan(one_expert, jnp.zeros((TOKEN_COUNT, D), jnp.float32), jnp.arange(EXPERTS, dtype=jnp.int32))
    return summed

def reference(queries, key_rows, value_rows, cum_gate, residual, out_weight, gain_mix, gain_pre, gain_post, route_ids, route_weight, w_gate, w_up, w_down):
    attended = attention(queries, key_rows, value_rows, cum_gate)
    projected = jnp.dot(attended, out_weight, preferred_element_type=jnp.float32)
    stream = (residual.astype(jnp.float32) + rms_scale(projected, gain_mix)).astype(jnp.bfloat16)
    stream_wide = lax.optimization_barrier(stream).astype(jnp.float32)
    normed = rms_scale(stream_wide, gain_pre).astype(jnp.bfloat16)
    combined = route_experts(normed, route_ids, route_weight, w_gate, w_up, w_down)
    return (stream_wide + rms_scale(combined, gain_post)).astype(jnp.bfloat16)
```

```python
import functools
import math

import jax
import jax.numpy as jnp
from jax import lax
from jax.experimental import pallas as pl
from jax.experimental.pallas import tpu as pltpu
from jax.sharding import PartitionSpec as P

HEAD_DIM = 64


NORM_EPS = 1e-06
MASKED = -1e30
LOG2E = math.log2(math.e)
MESH = pl.DeviceIdType.MESH
TILE = 256


def rms_scale(rows, gain):
    mean_sq = jnp.mean(rows * rows, axis=-1, keepdims=True)
    return rows * lax.rsqrt(mean_sq + NORM_EPS) * gain


def where(sp, tp):
    return dict(device_id=(sp, tp), device_id_type=MESH)


def attention_kernel(
    q_ref, kv_ref, gate_ref, out_ref,
    q_in, q_use, kv_buf, v_one, gate_buf, peak, acc, o_out, o_in,
    kv_send, kv_recv, fwd_send, fwd_recv, q_send, q_recv, gate_send, gate_recv, o_send, o_recv,
):
    tok = q_ref.shape[0]
    half = tok // 2
    sp, tp = lax.axis_index("sp"), lax.axis_index("tp")
    z, x = sp // 4, sp % 4
    y, core = tp // 2, tp % 2
    partner = 2 * y + (1 - core)
    bz, bx = z // 2, x // 2
    zl, xl = jnp.minimum(z, 3 - z), jnp.minimum(x, 3 - x)
    zh, xh = 3 - zl, 3 - xl
    top_block = 4 * zh + xh
    pair_of_me = jnp.abs(bz - bx)
    owner = core == bz
    low_block = 4 * zl + jnp.where(core == 0, xl, xh)
    blocks = (low_block, 15 - low_block)

    def copy(src, dst, send_sem, recv_sem, dev_sp, dev_tp):
        return pltpu.make_async_remote_copy(
            src_ref=src, dst_ref=dst, send_sem=send_sem, recv_sem=recv_sem, **where(dev_sp, dev_tp)
        )

    q_copies = []
    for side in range(2):
        dest_sp = 4 * jnp.where(core == 0, zl, zh) + (xl if side == 0 else xh)
        dest_tp = 2 * y + pair_of_me
        mine = (dest_sp == sp) & (dest_tp == tp)
        cp = copy(q_ref, q_in.at[bz], q_send.at[side], q_recv.at[bz], dest_sp, dest_tp)
        q_copies.append((mine, cp))

        @pl.when(jnp.logical_not(mine))
        def _():
            cp.start()

        @pl.when(mine)
        def _():
            q_in[bz] = q_ref[...]

    gate_cp = copy(gate_ref, gate_buf, gate_send, gate_recv, sp, partner)
    own_cp = copy(kv_ref.at[bx], kv_buf.at[0], fwd_send.at[0], fwd_recv.at[0], sp, partner)

    @pl.when(owner)
    def _():
        gate_cp.start()
        own_cp.start()
        gate_buf[...] = gate_ref[...]
        kv_buf[0] = kv_ref[bx]

    def kv_out(k, d):
        dz, dx = k // 4, k % 4
        dest_z, dest_x = (z - dz + 4) % 4, (x - dx + 4) % 4
        top = 4 * jnp.maximum(dest_z, 3 - dest_z) + jnp.maximum(dest_x, 3 - dest_x)
        used = (dest_z // 2 == core) & (sp <= top)
        rows = pl.ds(d * half, half)
        return used, copy(
            kv_ref.at[dest_x // 2, rows], kv_buf.at[k, rows], kv_send.at[k, d], kv_recv.at[k],
            4 * dest_z + dest_x, 2 * y + d,
        )

    def source(k):
        return 4 * ((z + k // 4) % 4) + (x + k % 4) % 4

    def send_kv(k, carry):
        for d in range(2):
            used, cp = kv_out(k, d)

            @pl.when(used)
            def _():
                cp.start()

        return carry

    lax.fori_loop(1, 16, send_kv, 0)

    def arrived(k):
        rows = pl.ds(core * half, half)
        return copy(kv_buf.at[k, rows], kv_buf.at[k, rows], kv_send.at[0, 0], kv_recv.at[k], sp, partner)

    def passed(k):
        rows = pl.ds(core * half, half)
        return copy(kv_buf.at[k, rows], kv_buf.at[k, rows], fwd_send.at[k], fwd_recv.at[k], sp, partner)

    def expected(k):
        rows = pl.ds((1 - core) * half, half)
        return copy(kv_buf.at[k, rows], kv_buf.at[k, rows], fwd_send.at[k], fwd_recv.at[k], sp, partner)

    @pl.when(jnp.logical_not(owner))
    def _():
        gate_cp.wait_recv()

    peak[...] = jnp.full_like(peak, MASKED)
    acc[...] = jnp.zeros_like(acc)
    lane = lax.broadcasted_iota(jnp.int32, (TILE, 128), 1)
    for slot in range(2):
        from_x = jnp.where(core == slot, xl, xh)
        from_sp = 4 * (zl if slot == 0 else zh) + from_x
        local = (from_sp == sp) & owner

        @pl.when(jnp.logical_not(local))
        def _():
            copy(q_ref, q_in.at[slot], q_send.at[0], q_recv.at[slot], sp, partner).wait_recv()

        for r in range(tok // TILE):
            rows = pl.ds(r * TILE, TILE)
            wide = q_in[slot, rows, :].astype(jnp.float32) * (HEAD_DIM ** -0.5)
            wide = jnp.where(bx == 0, wide, pltpu.roll(wide, 64, 1))
            q_use[slot, rows, :] = jnp.where(lane < HEAD_DIM, wide, 0.0).astype(jnp.bfloat16)

    @pl.when(jnp.logical_not(owner))
    def _():
        own_cp.wait_recv()

    def tile(k, j, slot, row, keys, masked):
        rows = pl.ds(row, TILE)
        block = blocks[slot]
        base = gate_buf[bx, block, :, 0:1]
        bias = (base - gate_buf[bx, j, :, 0:keys]) * LOG2E
        s = lax.dot_general(
            q_use[slot, rows, :], kv_buf[k, 0:keys, :], (((1,), (1,)), ((), ())),
            preferred_element_type=jnp.float32,
        )
        s = s * LOG2E + bias
        if masked:
            q_pos = row + lax.broadcasted_iota(jnp.int32, (TILE, keys), 0)
            k_pos = lax.broadcasted_iota(jnp.int32, (TILE, keys), 1)
            s = jnp.where(k_pos <= q_pos, s, MASKED)
        old = peak[slot, rows, :]
        new = jnp.maximum(old, jnp.max(s, axis=1, keepdims=True))
        peak[slot, rows, :] = new
        p = jnp.exp2(s - new[:, 0:1]).astype(jnp.bfloat16)
        acc[slot, rows, :] = acc[slot, rows, :] * jnp.exp2(old - new) + jnp.dot(
            p, v_one[0:keys, :], preferred_element_type=jnp.float32
        )

    def step(k, carry):
        j = source(k)
        follow = source(k + 1)
        used = j <= top_block

        @pl.when((k < 15) & (follow <= top_block))
        def _():
            arrived(k + 1).wait_recv()
            passed(k + 1).start()

        @pl.when((k > 0) & used)
        def _():
            expected(k).wait_recv()

        @pl.when(used)
        def _():
            v_one[...] = jnp.where(
                lax.broadcasted_iota(jnp.int32, (tok, 128), 1) < HEAD_DIM,
                jnp.bfloat16(1.0), kv_buf[k],
            )

        for slot in range(2):
            @pl.when(j < blocks[slot])
            def _():
                def rows_of(r, c):
                    tile(k, j, slot, pl.multiple_of(r * TILE, TILE), tok, False)
                    return c

                lax.fori_loop(0, tok // TILE, rows_of, 0)

            @pl.when(j == blocks[slot])
            def _():
                for r in range(tok // TILE):
                    tile(k, j, slot, r * TILE, (r + 1) * TILE, True)

        return carry

    lax.fori_loop(0, 16, step, 0)

    lane64 = lax.broadcasted_iota(jnp.int32, (64, 128), 1)
    head = 4 * y + 2 * bz + bx

    def o_copy(slot, t):
        return copy(o_out.at[slot, t], o_in.at[head], o_send.at[slot, t], o_recv.at[head], blocks[slot], t)

    for slot in range(2):
        for t in range(8):
            o = acc[slot, t * 128:(t + 1) * 128, :]
            o = o / pltpu.roll(o, 64, 1)
            o_out[slot, t] = jnp.where(lane64 < 64, pltpu.roll(o[0:64], 64, 1), o[64:128]).astype(jnp.bfloat16)
    for slot in range(2):
        for t in range(8):
            mine = (blocks[slot] == sp) & (tp == t)

            @pl.when(mine)
            def _():
                o_in[head] = o_out[slot, t]

            @pl.when(jnp.logical_not(mine))
            def _():
                o_copy(slot, t).start()

    for h in range(16):
        r = h % 4
        from_z = zl if r < 2 else zh
        from_x = xl if r % 2 == 0 else xh
        mine = (4 * from_z + from_x == sp) & (2 * (h // 4) + pair_of_me == tp)

        @pl.when(jnp.logical_not(mine))
        def _():
            copy(o_out.at[0, 0], o_in.at[h], o_send.at[0, 0], o_recv.at[h], sp, partner).wait_recv()

    for h in range(0, 16, 2):
        a = o_in[h].astype(jnp.float32)
        b = o_in[h + 1].astype(jnp.float32)
        cols = slice(h * 64, h * 64 + 128)
        out_ref[0:64, cols] = jnp.where(lane64 < 64, a, pltpu.roll(b, 64, 1)).astype(jnp.bfloat16)
        out_ref[64:128, cols] = jnp.where(lane64 < 64, pltpu.roll(a, 64, 1), b).astype(jnp.bfloat16)

    for mine, cp in q_copies:
        @pl.when(jnp.logical_not(mine))
        def _():
            cp.wait_send()

    @pl.when(owner)
    def _():
        gate_cp.wait_send()
        own_cp.wait_send()

    def drain(k, carry):
        for d in range(2):
            used, cp = kv_out(k, d)

            @pl.when(used)
            def _():
                cp.wait_send()

        @pl.when(source(k) <= top_block)
        def _():
            passed(k).wait_send()

        return carry

    lax.fori_loop(1, 16, drain, 0)
    for slot in range(2):
        for t in range(8):
            @pl.when(jnp.logical_not((blocks[slot] == sp) & (tp == t)))
            def _():
                o_copy(slot, t).wait_send()


def attention(queries, key_rows, value_rows, cum_gate):
    tok = queries.shape[0]
    kv = jnp.stack([
        jnp.concatenate([key_rows[:, :64], value_rows[:, :64]], axis=1),
        jnp.concatenate([key_rows[:, 64:], value_rows[:, 64:]], axis=1),
    ])
    gate = cum_gate.reshape(2, 16, 1, tok)
    dma = pltpu.SemaphoreType.DMA
    return pl.pallas_call(
        attention_kernel,
        out_shape=jax.ShapeDtypeStruct((128, 1024), jnp.bfloat16),
        in_specs=[pl.BlockSpec(memory_space=pltpu.VMEM)] * 3,
        out_specs=pl.BlockSpec(memory_space=pltpu.VMEM),
        scratch_shapes=[
            pltpu.VMEM((2, tok, 128), jnp.bfloat16),
            pltpu.VMEM((2, tok, 128), jnp.bfloat16),
            pltpu.VMEM((16, tok, 128), jnp.bfloat16),
            pltpu.VMEM((tok, 128), jnp.bfloat16),
            pltpu.VMEM((2, 16, 1, tok), jnp.float32),
            pltpu.VMEM((2, tok, 128), jnp.float32),
            pltpu.VMEM((2, tok, 128), jnp.float32),
            pltpu.VMEM((2, 8, 64, 128), jnp.bfloat16),
            pltpu.VMEM((16, 64, 128), jnp.bfloat16),
            dma((16, 2)), dma((16,)), dma((16,)), dma((16,)), dma((2,)), dma((2,)), dma, dma,
            dma((2, 8)), dma((16,)),
        ],
        compiler_params=pltpu.CompilerParams(has_side_effects=True, vmem_limit_bytes=40 * 1024 * 1024),
        name="attention",
    )(queries, kv, gate)


def local(
    queries,
    key_rows,
    value_rows,
    cum_gate,
    residual,
    out_weight,
    gain_mix,
    gain_pre,
    gain_post,
    route_ids,
    route_weight,
    w_gate,
    w_up,
    w_down,
):
    head_rows = attention(queries, key_rows, value_rows, cum_gate)
    projected = jnp.dot(head_rows, out_weight, preferred_element_type=jnp.float32)
    stream = (residual.astype(jnp.float32) + rms_scale(projected, gain_mix)).astype(jnp.bfloat16)
    stream_wide = lax.optimization_barrier(stream).astype(jnp.float32)
    normed = rms_scale(stream_wide, gain_pre).astype(jnp.bfloat16)
    rows_dev, top_count = route_ids.shape
    model_width = normed.shape[1]
    experts_all = lax.axis_size("sp") * lax.axis_size("tp")
    capacity = max(2, (4 * rows_dev * top_count + 3 * experts_all - 1) // (3 * experts_all))
    flat_ids = route_ids.reshape(-1)
    onehot = (flat_ids[:, None] == lax.iota(jnp.int32, experts_all)[None, :]).astype(jnp.int32)
    slot_rank = jnp.sum(jnp.cumsum(onehot, axis=0) * onehot, axis=1) - 1
    slot_index = flat_ids * capacity + slot_rank
    spread = jnp.repeat(normed, top_count, axis=0)
    outgoing = (
        jnp.zeros((experts_all * capacity, model_width), jnp.bfloat16).at[slot_index].set(spread)
    )
    outgoing = outgoing.reshape(experts_all, capacity, model_width)
    arrived = lax.all_to_all(outgoing, ("sp", "tp"), split_axis=0, concat_axis=0, tiled=True)
    sources, slots, width_here = arrived.shape
    flat_rows = arrived.reshape(sources * slots, width_here)
    gate_act = jnp.dot(flat_rows, w_gate[0], preferred_element_type=jnp.float32)
    up_act = jnp.dot(flat_rows, w_up[0], preferred_element_type=jnp.float32)
    hidden = (jax.nn.silu(gate_act) * up_act).astype(jnp.bfloat16)
    expert_out = jnp.dot(hidden, w_down[0], preferred_element_type=jnp.float32).astype(jnp.bfloat16)
    returned = lax.all_to_all(
        expert_out.reshape(sources, slots, width_here),
        ("sp", "tp"),
        split_axis=0,
        concat_axis=0,
        tiled=True,
    )
    picked = returned.reshape(experts_all * capacity, model_width)[slot_index]
    picked = picked.reshape(rows_dev, top_count, model_width).astype(jnp.float32)
    combined = jnp.sum(picked * route_weight[:, :, None], axis=1)
    return (stream_wide + rms_scale(combined, gain_post)).astype(jnp.bfloat16)


def solution(mesh):
    return jax.shard_map(
        local,
        mesh=mesh,
        in_specs=(
            P("sp", "tp"),
            P("sp", "tp"),
            P("sp", "tp"),
            P("tp", None),
            P(("sp", "tp"), None),
            P(),
            P(),
            P(),
            P(),
            P(("sp", "tp"), None),
            P(("sp", "tp"), None),
            P(("sp", "tp"), None, None),
            P(("sp", "tp"), None, None),
            P(("sp", "tp"), None, None),
        ),
        out_specs=P(("sp", "tp"), None),
        check_vma=False,
    )
```

```python
import functools
import math

import jax
import jax.numpy as jnp
from jax import lax
from jax.experimental import pallas as pl
from jax.experimental.pallas import tpu as pltpu
from jax.sharding import PartitionSpec as P

HEAD_DIM = 64


NORM_EPS = 1e-06
MASKED = -1e30
LOG2E = math.log2(math.e)
MESH = pl.DeviceIdType.MESH
TILE = 256
SLOTS = 3
GROUP = 32


def rms_scale(rows, gain):
    mean_sq = jnp.mean(rows * rows, axis=-1, keepdims=True)
    return rows * lax.rsqrt(mean_sq + NORM_EPS) * gain


def where(sp, tp):
    return dict(device_id=(sp, tp), device_id_type=MESH)


def offset_of(place):
    low, mid, high = place % 4, (place // 4) % 4, (place // 16) % 4
    return low, (mid + low) % 4, (high + mid + low) % 4, place // 64


def place_of(dz, dx, dy, dcore):
    mid = (dx - dz + 4) % 4
    high = (dy - dz - mid + 8) % 4
    return dz + 4 * mid + 16 * high + 64 * dcore


def layer_kernel(
    q_ref, kv_ref, gate_ref, residual_ref, mix_ref, pre_ref, post_ref,
    token_ref, place_ref, weight_ref, ow_hbm, wg_hbm, wu_hbm, wd_hbm, out_ref,
    q_in, q_use, kv_buf, v_one, gate_buf, peak, acc, o_out, o_in, att,
    ow, wg, wu, wd, slab_wide, slab, stream, outgoing, arrived_rows, results, returned,
    x_wide, x_rows, y_wide,
    kv_send, kv_recv, fwd_send, fwd_recv, q_send, q_recv, gate_send, gate_recv, o_send, o_recv,
    w_sem, go_send, go_recv, back_send, back_recv,
):
    tok = q_ref.shape[0]
    half = tok // 2
    sp, tp = lax.axis_index("sp"), lax.axis_index("tp")
    z, x = sp // 4, sp % 4
    y, core = tp // 2, tp % 2
    partner = 2 * y + (1 - core)
    bz, bx = z // 2, x // 2
    zl, xl = jnp.minimum(z, 3 - z), jnp.minimum(x, 3 - x)
    zh, xh = 3 - zl, 3 - xl
    top_block = 4 * zh + xh
    pair_of_me = jnp.abs(bz - bx)
    owner = core == bz
    low_block = 4 * zl + jnp.where(core == 0, xl, xh)
    blocks = (low_block, 15 - low_block)

    def copy(src, dst, send_sem, recv_sem, dev_sp, dev_tp):
        return pltpu.make_async_remote_copy(
            src_ref=src, dst_ref=dst, send_sem=send_sem, recv_sem=recv_sem, **where(dev_sp, dev_tp)
        )

    loads = [
        pltpu.make_async_copy(src, dst, w_sem.at[i])
        for i, (src, dst) in enumerate(((ow_hbm, ow), (wg_hbm, wg), (wu_hbm, wu), (wd_hbm, wd)))
    ]
    for load in loads:
        load.start()

    q_copies = []
    for side in range(2):
        dest_sp = 4 * jnp.where(core == 0, zl, zh) + (xl if side == 0 else xh)
        dest_tp = 2 * y + pair_of_me
        mine = (dest_sp == sp) & (dest_tp == tp)
        cp = copy(q_ref, q_in.at[bz], q_send.at[side], q_recv.at[bz], dest_sp, dest_tp)
        q_copies.append((mine, cp))

        @pl.when(jnp.logical_not(mine))
        def _():
            cp.start()

        @pl.when(mine)
        def _():
            q_in[bz] = q_ref[...]

    gate_cp = copy(gate_ref, gate_buf, gate_send, gate_recv, sp, partner)
    own_cp = copy(kv_ref.at[bx], kv_buf.at[0], fwd_send.at[0], fwd_recv.at[0], sp, partner)

    @pl.when(owner)
    def _():
        gate_cp.start()
        own_cp.start()
        gate_buf[...] = gate_ref[...]
        kv_buf[0] = kv_ref[bx]

    def kv_out(k, d):
        dz, dx = k // 4, k % 4
        dest_z, dest_x = (z - dz + 4) % 4, (x - dx + 4) % 4
        top = 4 * jnp.maximum(dest_z, 3 - dest_z) + jnp.maximum(dest_x, 3 - dest_x)
        used = (dest_z // 2 == core) & (sp <= top)
        rows = pl.ds(d * half, half)
        return used, copy(
            kv_ref.at[dest_x // 2, rows], kv_buf.at[k, rows], kv_send.at[k, d], kv_recv.at[k],
            4 * dest_z + dest_x, 2 * y + d,
        )

    def source(k):
        return 4 * ((z + k // 4) % 4) + (x + k % 4) % 4

    def send_kv(k, carry):
        for d in range(2):
            used, cp = kv_out(k, d)

            @pl.when(used)
            def _():
                cp.start()

        return carry

    lax.fori_loop(1, 16, send_kv, 0)

    def arrived(k):
        rows = pl.ds(core * half, half)
        return copy(kv_buf.at[k, rows], kv_buf.at[k, rows], kv_send.at[0, 0], kv_recv.at[k], sp, partner)

    def passed(k):
        rows = pl.ds(core * half, half)
        return copy(kv_buf.at[k, rows], kv_buf.at[k, rows], fwd_send.at[k], fwd_recv.at[k], sp, partner)

    def expected(k):
        rows = pl.ds((1 - core) * half, half)
        return copy(kv_buf.at[k, rows], kv_buf.at[k, rows], fwd_send.at[k], fwd_recv.at[k], sp, partner)

    @pl.when(jnp.logical_not(owner))
    def _():
        gate_cp.wait_recv()

    peak[...] = jnp.full_like(peak, MASKED)
    acc[...] = jnp.zeros_like(acc)
    lane = lax.broadcasted_iota(jnp.int32, (TILE, 128), 1)
    for slot in range(2):
        from_x = jnp.where(core == slot, xl, xh)
        from_sp = 4 * (zl if slot == 0 else zh) + from_x
        local = (from_sp == sp) & owner

        @pl.when(jnp.logical_not(local))
        def _():
            copy(q_ref, q_in.at[slot], q_send.at[0], q_recv.at[slot], sp, partner).wait_recv()

        for r in range(tok // TILE):
            rows = pl.ds(r * TILE, TILE)
            wide = q_in[slot, rows, :].astype(jnp.float32) * (HEAD_DIM ** -0.5)
            wide = jnp.where(bx == 0, wide, pltpu.roll(wide, 64, 1))
            q_use[slot, rows, :] = jnp.where(lane < HEAD_DIM, wide, 0.0).astype(jnp.bfloat16)

    @pl.when(jnp.logical_not(owner))
    def _():
        own_cp.wait_recv()

    def tile(k, j, slot, row, keys, masked):
        rows = pl.ds(row, TILE)
        block = blocks[slot]
        base = gate_buf[bx, block, :, 0:1]
        bias = (base - gate_buf[bx, j, :, 0:keys]) * LOG2E
        s = lax.dot_general(
            q_use[slot, rows, :], kv_buf[k, 0:keys, :], (((1,), (1,)), ((), ())),
            preferred_element_type=jnp.float32,
        )
        s = s * LOG2E + bias
        if masked:
            q_pos = row + lax.broadcasted_iota(jnp.int32, (TILE, keys), 0)
            k_pos = lax.broadcasted_iota(jnp.int32, (TILE, keys), 1)
            s = jnp.where(k_pos <= q_pos, s, MASKED)
        old = peak[slot, rows, :]
        new = jnp.maximum(old, jnp.max(s, axis=1, keepdims=True))
        peak[slot, rows, :] = new
        p = jnp.exp2(s - new[:, 0:1]).astype(jnp.bfloat16)
        acc[slot, rows, :] = acc[slot, rows, :] * jnp.exp2(old - new) + jnp.dot(
            p, v_one[0:keys, :], preferred_element_type=jnp.float32
        )

    def step(k, carry):
        j = source(k)
        follow = source(k + 1)
        used = j <= top_block

        @pl.when((k < 15) & (follow <= top_block))
        def _():
            arrived(k + 1).wait_recv()
            passed(k + 1).start()

        @pl.when((k > 0) & used)
        def _():
            expected(k).wait_recv()

        @pl.when(used)
        def _():
            v_one[...] = jnp.where(
                lax.broadcasted_iota(jnp.int32, (tok, 128), 1) < HEAD_DIM,
                jnp.bfloat16(1.0), kv_buf[k],
            )

        for slot in range(2):
            @pl.when(j < blocks[slot])
            def _():
                def rows_of(r, c):
                    tile(k, j, slot, pl.multiple_of(r * TILE, TILE), tok, False)
                    return c

                lax.fori_loop(0, tok // TILE, rows_of, 0)

            @pl.when(j == blocks[slot])
            def _():
                for r in range(tok // TILE):
                    tile(k, j, slot, r * TILE, (r + 1) * TILE, True)

        return carry

    lax.fori_loop(0, 16, step, 0)

    lane64 = lax.broadcasted_iota(jnp.int32, (64, 128), 1)
    head = 4 * y + 2 * bz + bx

    def o_copy(slot, t):
        return copy(o_out.at[slot, t], o_in.at[head], o_send.at[slot, t], o_recv.at[head], blocks[slot], t)

    for slot in range(2):
        for t in range(8):
            o = acc[slot, t * 128:(t + 1) * 128, :]
            o = o / pltpu.roll(o, 64, 1)
            o_out[slot, t] = jnp.where(lane64 < 64, pltpu.roll(o[0:64], 64, 1), o[64:128]).astype(jnp.bfloat16)
    for slot in range(2):
        for t in range(8):
            mine = (blocks[slot] == sp) & (tp == t)

            @pl.when(mine)
            def _():
                o_in[head] = o_out[slot, t]

            @pl.when(jnp.logical_not(mine))
            def _():
                o_copy(slot, t).start()

    for h in range(16):
        r = h % 4
        from_z = zl if r < 2 else zh
        from_x = xl if r % 2 == 0 else xh
        mine = (4 * from_z + from_x == sp) & (2 * (h // 4) + pair_of_me == tp)

        @pl.when(jnp.logical_not(mine))
        def _():
            copy(o_out.at[0, 0], o_in.at[h], o_send.at[0, 0], o_recv.at[h], sp, partner).wait_recv()

    for h in range(0, 16, 2):
        a = o_in[h].astype(jnp.float32)
        b = o_in[h + 1].astype(jnp.float32)
        cols = slice(h * 64, h * 64 + 128)
        att[0:64, cols] = jnp.where(lane64 < 64, a, pltpu.roll(b, 64, 1)).astype(jnp.bfloat16)
        att[64:128, cols] = jnp.where(lane64 < 64, pltpu.roll(a, 64, 1), b).astype(jnp.bfloat16)

    loads[0].wait()
    projected = jnp.dot(att[...], ow[...], preferred_element_type=jnp.float32)
    rows_in = residual_ref[...].astype(jnp.float32) + rms_scale(projected, mix_ref[...])
    rows_in = rows_in.astype(jnp.bfloat16).astype(jnp.float32)
    stream[...] = rows_in
    normed = rms_scale(rows_in, pre_ref[...])
    for c in range(16):
        slab_wide[pl.ds(c, 128, stride=16), :] = normed[:, c * 128:(c + 1) * 128]
    slab[...] = slab_wide[...].reshape(128, 16, 128).astype(jnp.bfloat16)

    def fill(place, carry):
        for s in range(SLOTS):
            outgoing[place * SLOTS + s] = slab[token_ref[place * SLOTS + s]]
        return carry

    lax.fori_loop(0, 128, fill, 0, unroll=4)

    def peer(place, sign):
        dz, dx, dy, dcore = offset_of(place)
        return (
            4 * ((z + sign * dz + 4) % 4) + (x + sign * dx + 4) % 4,
            2 * ((y + sign * dy + 4) % 4) + (core + dcore) % 2,
        )

    def go(place):
        rows = pl.ds(place * SLOTS, SLOTS)
        return copy(
            outgoing.at[rows], arrived_rows.at[rows], go_send, go_recv.at[place // GROUP], *peer(place, 1)
        )

    def back(place):
        rows = pl.ds(place * SLOTS, SLOTS)
        return copy(
            results.at[rows], returned.at[rows], back_send, back_recv.at[place // GROUP], *peer(place, -1)
        )

    def start_go(place, carry):
        go(place).start()
        return carry

    lax.fori_loop(1, 128, start_go, 0)
    arrived_rows[0:SLOTS] = outgoing[0:SLOTS]
    for load in loads[1:]:
        load.wait()

    def group_rows(group):
        first = SLOTS if group == 0 else group * GROUP * SLOTS
        return pl.ds(first, (group + 1) * GROUP * SLOTS - first)

    def expert_group(group):
        rows = group_rows(group)
        copy(
            outgoing.at[rows], arrived_rows.at[rows], go_send, go_recv.at[group], sp, partner
        ).wait_recv()
        count = GROUP * SLOTS
        first = group * count
        x_wide[...] = arrived_rows[first:first + count].reshape(count * 16, 128).astype(jnp.float32)
        for c in range(16):
            x_rows[:, c * 128:(c + 1) * 128] = x_wide[pl.ds(c, count, stride=16), :].astype(jnp.bfloat16)
        gate_act = jnp.dot(x_rows[...], wg[...], preferred_element_type=jnp.float32)
        up_act = jnp.dot(x_rows[...], wu[...], preferred_element_type=jnp.float32)
        hidden = (gate_act / (1.0 + jnp.exp(-gate_act)) * up_act).astype(jnp.bfloat16)
        y = jnp.dot(hidden, wd[...], preferred_element_type=jnp.float32)
        for c in range(16):
            y_wide[pl.ds(c, count, stride=16), :] = y[:, c * 128:(c + 1) * 128]
        results[first:first + count] = y_wide[...].reshape(count, 16, 128).astype(jnp.bfloat16)

        def start_back(place, carry):
            back(place).start()
            return carry

        lax.fori_loop(max(1, group * GROUP), (group + 1) * GROUP, start_back, 0)
        if group == 0:
            returned[0:SLOTS] = results[0:SLOTS]

    for group in range(128 // GROUP):
        expert_group(group)
    for group in range(128 // GROUP):
        rows = group_rows(group)
        copy(
            results.at[rows], returned.at[rows], back_send, back_recv.at[group], sp, partner
        ).wait_recv()

    def combine(n, carry):
        first = returned[place_ref[n, 0]].astype(jnp.float32) * weight_ref[n, 0]
        second = returned[place_ref[n, 1]].astype(jnp.float32) * weight_ref[n, 1]
        slab_wide[pl.ds(pl.multiple_of(n * 16, 16), 16), :] = first + second
        return carry

    lax.fori_loop(0, 128, combine, 0, unroll=4)
    combined = jnp.concatenate(
        [slab_wide[pl.ds(c, 128, stride=16), :] for c in range(16)], axis=1
    )
    out_ref[...] = (stream[...] + rms_scale(combined, post_ref[...])).astype(jnp.bfloat16)

    for mine, cp in q_copies:
        @pl.when(jnp.logical_not(mine))
        def _():
            cp.wait_send()

    @pl.when(owner)
    def _():
        gate_cp.wait_send()
        own_cp.wait_send()

    def drain(k, carry):
        for d in range(2):
            used, cp = kv_out(k, d)

            @pl.when(used)
            def _():
                cp.wait_send()

        @pl.when(source(k) <= top_block)
        def _():
            passed(k).wait_send()

        return carry

    lax.fori_loop(1, 16, drain, 0)
    for slot in range(2):
        for t in range(8):
            @pl.when(jnp.logical_not((blocks[slot] == sp) & (tp == t)))
            def _():
                o_copy(slot, t).wait_send()
    everything = pl.ds(SLOTS, 127 * SLOTS)
    copy(outgoing.at[everything], arrived_rows.at[everything], go_send, go_recv.at[0], sp, partner).wait_send()
    copy(results.at[everything], returned.at[everything], back_send, back_recv.at[0], sp, partner).wait_send()


def local(
    queries,
    key_rows,
    value_rows,
    cum_gate,
    residual,
    out_weight,
    gain_mix,
    gain_pre,
    gain_post,
    route_ids,
    route_weight,
    w_gate,
    w_up,
    w_down,
):
    tok = queries.shape[0]
    kv = jnp.stack([
        jnp.concatenate([key_rows[:, :64], value_rows[:, :64]], axis=1),
        jnp.concatenate([key_rows[:, 64:], value_rows[:, 64:]], axis=1),
    ])
    gate = cum_gate.reshape(2, 16, 1, tok)
    sp, tp = lax.axis_index("sp"), lax.axis_index("tp")
    flat = route_ids.reshape(-1)
    order = lax.iota(jnp.int32, flat.shape[0])
    earlier = (flat[None, :] == flat[:, None]) & (order[None, :] < order[:, None])
    rank = jnp.sum(earlier.astype(jnp.int32), axis=1)
    e_sp, e_tp = flat // 8, flat % 8
    place = place_of(
        (e_sp // 4 - sp // 4 + 4) % 4,
        (e_sp % 4 - sp % 4 + 4) % 4,
        (e_tp // 2 - tp // 2 + 4) % 4,
        (e_tp % 2 + tp % 2) % 2,
    ) * SLOTS + rank
    slots = lax.iota(jnp.int32, 128 * SLOTS)
    token = jnp.sum(jnp.where(slots[:, None] == place[None, :], order[None, :] // 2, 0), axis=1)
    dma = pltpu.SemaphoreType.DMA
    vmem, smem, anywhere = (
        pl.BlockSpec(memory_space=space) for space in (pltpu.VMEM, pltpu.SMEM, pl.ANY)
    )
    bf16, f32 = jnp.bfloat16, jnp.float32
    rows = GROUP * SLOTS
    return pl.pallas_call(
        layer_kernel,
        out_shape=jax.ShapeDtypeStruct((128, 2048), bf16),
        in_specs=[vmem] * 7 + [smem] * 3 + [anywhere] * 4,
        out_specs=vmem,
        scratch_shapes=[
            pltpu.VMEM((2, tok, 128), bf16),
            pltpu.VMEM((2, tok, 128), bf16),
            pltpu.VMEM((16, tok, 128), bf16),
            pltpu.VMEM((tok, 128), bf16),
            pltpu.VMEM((2, 16, 1, tok), f32),
            pltpu.VMEM((2, tok, 128), f32),
            pltpu.VMEM((2, tok, 128), f32),
            pltpu.VMEM((2, 8, 64, 128), bf16),
            pltpu.VMEM((16, 64, 128), bf16),
            pltpu.VMEM((128, 1024), bf16),
            pltpu.VMEM((1024, 2048), bf16),
            pltpu.VMEM((2048, 512), bf16),
            pltpu.VMEM((2048, 512), bf16),
            pltpu.VMEM((512, 2048), bf16),
            pltpu.VMEM((2048, 128), f32),
            pltpu.VMEM((128, 16, 128), bf16),
            pltpu.VMEM((128, 2048), f32),
            pltpu.VMEM((128 * SLOTS, 16, 128), bf16),
            pltpu.VMEM((128 * SLOTS, 16, 128), bf16),
            pltpu.VMEM((128 * SLOTS, 16, 128), bf16),
            pltpu.VMEM((128 * SLOTS, 16, 128), bf16),
            pltpu.VMEM((rows * 16, 128), f32),
            pltpu.VMEM((rows, 2048), bf16),
            pltpu.VMEM((rows * 16, 128), f32),
            dma((16, 2)), dma((16,)), dma((16,)), dma((16,)), dma((2,)), dma((2,)), dma, dma,
            dma((2, 8)), dma((16,)),
            dma((4,)), dma, dma((128 // GROUP,)), dma, dma((128 // GROUP,)),
        ],
        compiler_params=pltpu.CompilerParams(has_side_effects=True, vmem_limit_bytes=60 * 1024 * 1024),
        name="layer",
    )(
        queries, kv, gate, residual, gain_mix.reshape(1, -1), gain_pre.reshape(1, -1),
        gain_post.reshape(1, -1), token, place.reshape(128, 2), route_weight,
        out_weight, w_gate[0], w_up[0], w_down[0],
    )


def solution(mesh):
    return jax.shard_map(
        local,
        mesh=mesh,
        in_specs=(
            P("sp", "tp"),
            P("sp", "tp"),
            P("sp", "tp"),
            P("tp", None),
            P(("sp", "tp"), None),
            P(),
            P(),
            P(),
            P(),
            P(("sp", "tp"), None),
            P(("sp", "tp"), None),
            P(("sp", "tp"), None, None),
            P(("sp", "tp"), None, None),
            P(("sp", "tp"), None, None),
        ),
        out_specs=P(("sp", "tp"), None),
        check_vma=False,
    )
```

```python
import functools
import math

import jax
import jax.numpy as jnp
from jax import lax
from jax.experimental import pallas as pl
from jax.experimental.pallas import tpu as pltpu
from jax.sharding import PartitionSpec as P

HEAD_DIM = 64


NORM_EPS = 1e-06
MASKED = -1e30
LOG2E = math.log2(math.e)
MESH = pl.DeviceIdType.MESH
TILE = 256
QROWS = 256
SLOTS = 3
GROUP = 32


def rms_scale(rows, gain):
    mean_sq = jnp.mean(rows * rows, axis=-1, keepdims=True)
    return rows * lax.rsqrt(mean_sq + NORM_EPS) * gain


def split3(values):
    first = values.astype(jnp.bfloat16).astype(jnp.float32)
    second = (values - first).astype(jnp.bfloat16).astype(jnp.float32)
    third = (values - first - second).astype(jnp.bfloat16).astype(jnp.float32)
    return first, second, third


def where(sp, tp):
    return dict(device_id=(sp, tp), device_id_type=MESH)


def offset_of(place):
    low, mid, high = place % 4, (place // 4) % 4, (place // 16) % 4
    return low, (mid + low) % 4, (high + mid + low) % 4, place // 64


def place_of(dz, dx, dy, dcore):
    mid = (dx - dz + 4) % 4
    high = (dy - dz - mid + 8) % 4
    return dz + 4 * mid + 16 * high + 64 * dcore


def layer_kernel(
    q_ref, kv_ref, gate_ref, residual_ref, mix_ref, pre_ref, post_ref,
    token_ref, place_ref, weight_ref, ow_hbm, wg_hbm, wu_hbm, wd_hbm, out_ref,
    q_in, q_use, kv_buf, gate_cols, k_aug, s_buf, v_one, gate_buf, peak, acc, o_out, o_in, att,
    ow, wg, wu, wd, slab_wide, slab, stream, outgoing, arrived_rows, results, returned,
    x_wide, x_rows, y_wide,
    kv_send, kv_recv, fwd_send, fwd_recv, q_send, q_recv, gate_send, gate_recv, o_send, o_recv,
    w_sem, go_send, go_recv, back_send, back_recv,
):
    tok = kv_ref.shape[1]
    half = tok // 2
    sp, tp = lax.axis_index("sp"), lax.axis_index("tp")
    z, x = sp // 4, sp % 4
    y, core = tp // 2, tp % 2
    partner = 2 * y + (1 - core)
    bz, bx = z // 2, x // 2
    zl, xl = jnp.minimum(z, 3 - z), jnp.minimum(x, 3 - x)
    zh, xh = 3 - zl, 3 - xl
    top_block = 4 * zh + xh
    pair_of_me = jnp.abs(bz - bx)
    owner = core == bz
    low_block = 4 * zl + jnp.where(core == 0, xl, xh)
    blocks = (low_block, 15 - low_block)

    def copy(src, dst, send_sem, recv_sem, dev_sp, dev_tp):
        return pltpu.make_async_remote_copy(
            src_ref=src, dst_ref=dst, send_sem=send_sem, recv_sem=recv_sem, **where(dev_sp, dev_tp)
        )

    loads = [
        pltpu.make_async_copy(src, dst, w_sem.at[i])
        for i, (src, dst) in enumerate(((ow_hbm, ow), (wg_hbm, wg), (wu_hbm, wu), (wd_hbm, wd)))
    ]
    for load in loads:
        load.start()

    q_copies = []
    for side in range(2):
        dest_sp = 4 * jnp.where(core == 0, zl, zh) + (xl if side == 0 else xh)
        dest_tp = 2 * y + pair_of_me
        mine = (dest_sp == sp) & (dest_tp == tp)
        cp = copy(q_ref.at[side], q_in.at[bz], q_send.at[side], q_recv.at[bz], dest_sp, dest_tp)
        q_copies.append((mine, cp))

        @pl.when(jnp.logical_not(mine))
        def _():
            cp.start()

        @pl.when(mine)
        def _():
            q_in[bz] = q_ref[side]

    gate_cp = copy(gate_ref, gate_buf, gate_send, gate_recv, sp, partner)
    own_cp = copy(kv_ref.at[bx], kv_buf.at[0], fwd_send.at[0], fwd_recv.at[0], sp, partner)

    @pl.when(owner)
    def _():
        gate_cp.start()
        own_cp.start()
        gate_buf[...] = gate_ref[...]
        kv_buf[0] = kv_ref[bx]

    def step_offset(k):
        return (-1369213168 >> (2 * k)) & 3, (-1182141244 >> (2 * k)) & 3

    def kv_out(k, d):
        dz, dx = step_offset(k)
        dest_z, dest_x = (z - dz + 4) % 4, (x - dx + 4) % 4
        top = 4 * jnp.maximum(dest_z, 3 - dest_z) + jnp.maximum(dest_x, 3 - dest_x)
        used = (dest_z // 2 == core) & (sp <= top)
        rows = pl.ds(d * half, half)
        return used, copy(
            kv_ref.at[dest_x // 2, rows], kv_buf.at[k, rows], kv_send.at[k, d], kv_recv.at[k],
            4 * dest_z + dest_x, 2 * y + d,
        )

    def source(k):
        dz, dx = step_offset(k)
        return 4 * ((z + dz) % 4) + (x + dx) % 4

    def send_kv(k, carry):
        for d in range(2):
            used, cp = kv_out(k, d)

            @pl.when(used)
            def _():
                cp.start()

        return carry

    lax.fori_loop(1, 9, send_kv, 0)

    def arrived(k):
        rows = pl.ds(core * half, half)
        return copy(kv_buf.at[k, rows], kv_buf.at[k, rows], kv_send.at[0, 0], kv_recv.at[k], sp, partner)

    def passed(k):
        rows = pl.ds(core * half, half)
        return copy(kv_buf.at[k, rows], kv_buf.at[k, rows], fwd_send.at[k], fwd_recv.at[k], sp, partner)

    def expected(k):
        rows = pl.ds((1 - core) * half, half)
        return copy(kv_buf.at[k, rows], kv_buf.at[k, rows], fwd_send.at[k], fwd_recv.at[k], sp, partner)

    @pl.when(jnp.logical_not(owner))
    def _():
        gate_cp.wait_recv()

    peak[...] = jnp.full_like(peak, MASKED)
    acc[...] = jnp.zeros_like(acc)
    lane = lax.broadcasted_iota(jnp.int32, (QROWS, 128), 1)
    at_row = lax.broadcasted_iota(jnp.int32, (8, 128), 0)
    at_lane = lax.broadcasted_iota(jnp.int32, (8, 128), 1)
    put = jnp.where(
        (at_lane == at_row + HEAD_DIM) & (at_row < 3) | (at_row == 3) & (at_lane >= HEAD_DIM + 3) & (at_lane < HEAD_DIM + 6),
        1.0, 0.0,
    ).astype(jnp.bfloat16)
    row8 = lax.broadcasted_iota(jnp.int32, (8, tok), 0)

    def columns(j, carry):
        parts = split3(gate_buf[bx, j] * -LOG2E)
        stack = jnp.where(row8 == 3, 1.0, 0.0)
        for i in range(3):
            stack = jnp.where(row8 == i, parts[i], stack)
        gate_cols[j] = lax.dot_general(
            stack.astype(jnp.bfloat16), put, (((0,), (0,)), ((), ())), preferred_element_type=jnp.float32
        ).astype(jnp.bfloat16)
        return carry

    lax.fori_loop(0, 16, columns, 0)
    for slot in range(2):
        from_x = jnp.where(core == slot, xl, xh)
        from_sp = 4 * (zl if slot == 0 else zh) + from_x
        local = (from_sp == sp) & owner

        @pl.when(jnp.logical_not(local))
        def _():
            copy(q_ref.at[0], q_in.at[slot], q_send.at[0], q_recv.at[slot], sp, partner).wait_recv()

        base = gate_buf[bx, blocks[slot], :, 0:1] * LOG2E
        pieces = split3(base)
        for r in range(tok // QROWS):
            rows = pl.ds(r * QROWS, QROWS)
            wide = q_in[slot, pl.ds(r * QROWS % half, QROWS), :].astype(jnp.float32) * (LOG2E * HEAD_DIM ** -0.5)
            wide = wide if r * QROWS < half else pltpu.roll(wide, 64, 1)
            high = jnp.where(lane < HEAD_DIM, wide, 0.0).astype(jnp.bfloat16)
            low = (wide - high.astype(jnp.float32)).astype(jnp.bfloat16).astype(jnp.float32)
            extra = jnp.where(lane < HEAD_DIM + 3, 1.0, 0.0)
            for i in range(3):
                extra = jnp.where(lane == HEAD_DIM + 3 + i, pieces[i], extra)
            q_use[slot, rows, 0:128] = high
            q_use[slot, rows, 128:256] = jnp.where(lane < HEAD_DIM, low, extra).astype(jnp.bfloat16)

    @pl.when(jnp.logical_not(owner))
    def _():
        own_cp.wait_recv()

    def attend(slot, diagonal):
        tiles = tok // TILE
        keys = [(r + 1) * TILE if diagonal else tok for r in range(tiles)]
        olds, news = [], []
        for i in range(tiles + 1):
            if i < tiles:
                rows = slice(i * TILE, (i + 1) * TILE)
                s = lax.dot_general(
                    q_use[slot, rows, :], k_aug[0:keys[i], :], (((1,), (1,)), ((), ())),
                    preferred_element_type=jnp.float32,
                )
                if diagonal:
                    q_pos = lax.broadcasted_iota(jnp.int32, (TILE, TILE), 0)
                    k_pos = lax.broadcasted_iota(jnp.int32, (TILE, TILE), 1)
                    last = jnp.where(k_pos <= q_pos, s[:, keys[i] - TILE:], MASKED)
                    s = last if i == 0 else jnp.concatenate([s[:, :keys[i] - TILE], last], axis=1)
                s_buf[i % s_buf.shape[0], :, 0:keys[i]] = s
                olds.append(peak[slot, rows, :])
                news.append(jnp.maximum(olds[i], jnp.max(s, axis=1, keepdims=True)))
                peak[slot, rows, :] = news[i]
            if i > 0:
                r = i - 1
                rows = slice(r * TILE, (r + 1) * TILE)
                p = jnp.exp2(s_buf[r % s_buf.shape[0], :, 0:keys[r]] - news[r][:, 0:1]).astype(jnp.bfloat16)
                acc[slot, rows, :] = acc[slot, rows, :] * jnp.exp2(olds[r] - news[r]) + jnp.dot(
                    p, v_one[0:keys[r], :], preferred_element_type=jnp.float32
                )

    def step(k, carry):
        @pl.when(k < 7)
        def _():
            send_kv(k + 9, 0)

        j = source(k)
        follow = source(jnp.minimum(k + 1, 15))
        used = j <= top_block

        @pl.when((k < 15) & (follow <= top_block))
        def _():
            arrived(k + 1).wait_recv()
            passed(k + 1).start()

        @pl.when((k > 0) & used)
        def _():
            expected(k).wait_recv()

        @pl.when(used)
        def _():
            left = lax.broadcasted_iota(jnp.int32, (tok, 128), 1) < HEAD_DIM
            rows_kv = kv_buf[k]
            v_one[...] = jnp.where(left, jnp.bfloat16(1.0), rows_kv)
            k_aug[:, 0:128] = rows_kv
            k_aug[:, 128:256] = jnp.where(left, rows_kv, gate_cols[j])

        for slot in range(2):
            @pl.when(j < blocks[slot])
            def _():
                attend(slot, False)

            @pl.when(j == blocks[slot])
            def _():
                attend(slot, True)

        return carry

    lax.fori_loop(0, 16, step, 0)

    lane64 = lax.broadcasted_iota(jnp.int32, (64, 128), 1)
    head = 4 * y + 2 * bz + bx

    def o_copy(slot, t):
        return copy(o_out.at[slot, t], o_in.at[head], o_send.at[slot, t], o_recv.at[head], blocks[slot], t)

    for slot in range(2):
        for t in range(8):
            o = acc[slot, t * 128:(t + 1) * 128, :]
            o = o / pltpu.roll(o, 64, 1)
            o_out[slot, t] = jnp.where(lane64 < 64, pltpu.roll(o[0:64], 64, 1), o[64:128]).astype(jnp.bfloat16)
    for slot in range(2):
        for t in range(8):
            mine = (blocks[slot] == sp) & (tp == t)

            @pl.when(mine)
            def _():
                o_in[head] = o_out[slot, t]

            @pl.when(jnp.logical_not(mine))
            def _():
                o_copy(slot, t).start()

    for h in range(16):
        r = h % 4
        from_z = zl if r < 2 else zh
        from_x = xl if r % 2 == 0 else xh
        mine = (4 * from_z + from_x == sp) & (2 * (h // 4) + pair_of_me == tp)

        @pl.when(jnp.logical_not(mine))
        def _():
            copy(o_out.at[0, 0], o_in.at[h], o_send.at[0, 0], o_recv.at[h], sp, partner).wait_recv()

    for h in range(0, 16, 2):
        a = o_in[h].astype(jnp.float32)
        b = o_in[h + 1].astype(jnp.float32)
        cols = slice(h * 64, h * 64 + 128)
        att[0:64, cols] = jnp.where(lane64 < 64, a, pltpu.roll(b, 64, 1)).astype(jnp.bfloat16)
        att[64:128, cols] = jnp.where(lane64 < 64, pltpu.roll(a, 64, 1), b).astype(jnp.bfloat16)

    loads[0].wait()
    projected = jnp.dot(att[...], ow[...], preferred_element_type=jnp.float32)
    rows_in = residual_ref[...].astype(jnp.float32) + rms_scale(projected, mix_ref[...])
    rows_in = rows_in.astype(jnp.bfloat16).astype(jnp.float32)
    stream[...] = rows_in
    normed = rms_scale(rows_in, pre_ref[...])
    for c in range(16):
        slab_wide[pl.ds(c, 128, stride=16), :] = normed[:, c * 128:(c + 1) * 128]
    slab[...] = slab_wide[...].reshape(128, 16, 128).astype(jnp.bfloat16)

    def fill(place, carry):
        for s in range(SLOTS):
            outgoing[place * SLOTS + s] = slab[token_ref[place * SLOTS + s]]
        return carry

    lax.fori_loop(0, 128, fill, 0, unroll=4)

    def peer(place, sign):
        dz, dx, dy, dcore = offset_of(place)
        return (
            4 * ((z + sign * dz + 4) % 4) + (x + sign * dx + 4) % 4,
            2 * ((y + sign * dy + 4) % 4) + (core + dcore) % 2,
        )

    def go(place):
        rows = pl.ds(place * SLOTS, SLOTS)
        return copy(
            outgoing.at[rows], arrived_rows.at[rows], go_send, go_recv.at[place // GROUP], *peer(place, 1)
        )

    def back(place):
        rows = pl.ds(place * SLOTS, SLOTS)
        return copy(
            results.at[rows], returned.at[rows], back_send, back_recv.at[place // GROUP], *peer(place, -1)
        )

    def start_go(place, carry):
        go(place).start()
        return carry

    lax.fori_loop(1, 128, start_go, 0)
    arrived_rows[0:SLOTS] = outgoing[0:SLOTS]
    for load in loads[1:]:
        load.wait()

    def group_rows(group):
        first = SLOTS if group == 0 else group * GROUP * SLOTS
        return pl.ds(first, (group + 1) * GROUP * SLOTS - first)

    def expert_group(group):
        rows = group_rows(group)
        copy(
            outgoing.at[rows], arrived_rows.at[rows], go_send, go_recv.at[group], sp, partner
        ).wait_recv()
        count = GROUP * SLOTS
        first = group * count
        x_wide[...] = arrived_rows[first:first + count].reshape(count * 16, 128).astype(jnp.float32)
        for c in range(16):
            x_rows[:, c * 128:(c + 1) * 128] = x_wide[pl.ds(c, count, stride=16), :].astype(jnp.bfloat16)
        gate_act = jnp.dot(x_rows[...], wg[...], preferred_element_type=jnp.float32)
        up_act = jnp.dot(x_rows[...], wu[...], preferred_element_type=jnp.float32)
        hidden = (gate_act / (1.0 + jnp.exp(-gate_act)) * up_act).astype(jnp.bfloat16)
        y = jnp.dot(hidden, wd[...], preferred_element_type=jnp.float32)
        for c in range(16):
            y_wide[pl.ds(c, count, stride=16), :] = y[:, c * 128:(c + 1) * 128]
        results[first:first + count] = y_wide[...].reshape(count, 16, 128).astype(jnp.bfloat16)

        def start_back(place, carry):
            back(place).start()
            return carry

        lax.fori_loop(max(1, group * GROUP), (group + 1) * GROUP, start_back, 0)
        if group == 0:
            returned[0:SLOTS] = results[0:SLOTS]

    for group in range(128 // GROUP):
        expert_group(group)
    for group in range(128 // GROUP):
        rows = group_rows(group)
        copy(
            results.at[rows], returned.at[rows], back_send, back_recv.at[group], sp, partner
        ).wait_recv()

    def combine(n, carry):
        first = returned[place_ref[n, 0]].astype(jnp.float32) * weight_ref[n, 0]
        second = returned[place_ref[n, 1]].astype(jnp.float32) * weight_ref[n, 1]
        slab_wide[pl.ds(pl.multiple_of(n * 16, 16), 16), :] = first + second
        return carry

    lax.fori_loop(0, 128, combine, 0, unroll=4)
    combined = jnp.concatenate(
        [slab_wide[pl.ds(c, 128, stride=16), :] for c in range(16)], axis=1
    )
    out_ref[...] = (stream[...] + rms_scale(combined, post_ref[...])).astype(jnp.bfloat16)

    for mine, cp in q_copies:
        @pl.when(jnp.logical_not(mine))
        def _():
            cp.wait_send()

    @pl.when(owner)
    def _():
        gate_cp.wait_send()
        own_cp.wait_send()

    def drain(k, carry):
        for d in range(2):
            used, cp = kv_out(k, d)

            @pl.when(used)
            def _():
                cp.wait_send()

        @pl.when(source(k) <= top_block)
        def _():
            passed(k).wait_send()

        return carry

    lax.fori_loop(1, 16, drain, 0)
    for slot in range(2):
        for t in range(8):
            @pl.when(jnp.logical_not((blocks[slot] == sp) & (tp == t)))
            def _():
                o_copy(slot, t).wait_send()
    everything = pl.ds(SLOTS, 127 * SLOTS)
    copy(outgoing.at[everything], arrived_rows.at[everything], go_send, go_recv.at[0], sp, partner).wait_send()
    copy(results.at[everything], returned.at[everything], back_send, back_recv.at[0], sp, partner).wait_send()


def local(
    queries,
    key_rows,
    value_rows,
    cum_gate,
    residual,
    out_weight,
    gain_mix,
    gain_pre,
    gain_post,
    route_ids,
    route_weight,
    w_gate,
    w_up,
    w_down,
):
    tok = queries.shape[0]
    kv = jnp.stack([
        jnp.concatenate([key_rows[:, :64], value_rows[:, :64]], axis=1),
        jnp.concatenate([key_rows[:, 64:], value_rows[:, 64:]], axis=1),
    ])
    packed = jnp.stack([
        jnp.concatenate([queries[:tok // 2, s:s + 64], queries[tok // 2:, s:s + 64]], axis=1) for s in (0, 64)
    ])
    gate = cum_gate.reshape(2, 16, 1, tok)
    sp, tp = lax.axis_index("sp"), lax.axis_index("tp")
    flat = route_ids.reshape(-1)
    order = lax.iota(jnp.int32, flat.shape[0])
    earlier = (flat[None, :] == flat[:, None]) & (order[None, :] < order[:, None])
    rank = jnp.sum(earlier.astype(jnp.int32), axis=1)
    e_sp, e_tp = flat // 8, flat % 8
    place = place_of(
        (e_sp // 4 - sp // 4 + 4) % 4,
        (e_sp % 4 - sp % 4 + 4) % 4,
        (e_tp // 2 - tp // 2 + 4) % 4,
        (e_tp % 2 + tp % 2) % 2,
    ) * SLOTS + rank
    slots = lax.iota(jnp.int32, 128 * SLOTS)
    token = jnp.sum(jnp.where(slots[:, None] == place[None, :], order[None, :] // 2, 0), axis=1)
    dma = pltpu.SemaphoreType.DMA
    vmem, smem, anywhere = (
        pl.BlockSpec(memory_space=space) for space in (pltpu.VMEM, pltpu.SMEM, pl.ANY)
    )
    bf16, f32 = jnp.bfloat16, jnp.float32
    rows = GROUP * SLOTS
    return pl.pallas_call(
        layer_kernel,
        out_shape=jax.ShapeDtypeStruct((128, 2048), bf16),
        in_specs=[vmem] * 7 + [smem] * 3 + [anywhere] * 4,
        out_specs=vmem,
        scratch_shapes=[
            pltpu.VMEM((2, tok // 2, 128), jnp.bfloat16),
            pltpu.VMEM((2, tok, 256), jnp.bfloat16),
            pltpu.VMEM((16, tok, 128), jnp.bfloat16),
            pltpu.VMEM((16, tok, 128), jnp.bfloat16),
            pltpu.VMEM((tok, 256), jnp.bfloat16),
            pltpu.VMEM((4, TILE, tok), jnp.float32),
            pltpu.VMEM((tok, 128), bf16),
            pltpu.VMEM((2, 16, 1, tok), f32),
            pltpu.VMEM((2, tok, 128), f32),
            pltpu.VMEM((2, tok, 128), f32),
            pltpu.VMEM((2, 8, 64, 128), bf16),
            pltpu.VMEM((16, 64, 128), bf16),
            pltpu.VMEM((128, 1024), bf16),
            pltpu.VMEM((1024, 2048), bf16),
            pltpu.VMEM((2048, 512), bf16),
            pltpu.VMEM((2048, 512), bf16),
            pltpu.VMEM((512, 2048), bf16),
            pltpu.VMEM((2048, 128), f32),
            pltpu.VMEM((128, 16, 128), bf16),
            pltpu.VMEM((128, 2048), f32),
            pltpu.VMEM((128 * SLOTS, 16, 128), bf16),
            pltpu.VMEM((128 * SLOTS, 16, 128), bf16),
            pltpu.VMEM((128 * SLOTS, 16, 128), bf16),
            pltpu.VMEM((128 * SLOTS, 16, 128), bf16),
            pltpu.VMEM((rows * 16, 128), f32),
            pltpu.VMEM((rows, 2048), bf16),
            pltpu.VMEM((rows * 16, 128), f32),
            dma((16, 2)), dma((16,)), dma((16,)), dma((16,)), dma((2,)), dma((2,)), dma, dma,
            dma((2, 8)), dma((16,)),
            dma((4,)), dma, dma((128 // GROUP,)), dma, dma((128 // GROUP,)),
        ],
        compiler_params=pltpu.CompilerParams(has_side_effects=True, vmem_limit_bytes=60 * 1024 * 1024),
        name="layer",
    )(
        packed, kv, gate, residual, gain_mix.reshape(1, -1), gain_pre.reshape(1, -1),
        gain_post.reshape(1, -1), token, place.reshape(128, 2), route_weight,
        out_weight, w_gate[0], w_up[0], w_down[0],
    )


def solution(mesh):
    return jax.shard_map(
        local,
        mesh=mesh,
        in_specs=(
            P("sp", "tp"),
            P("sp", "tp"),
            P("sp", "tp"),
            P("tp", None),
            P(("sp", "tp"), None),
            P(),
            P(),
            P(),
            P(),
            P(("sp", "tp"), None),
            P(("sp", "tp"), None),
            P(("sp", "tp"), None, None),
            P(("sp", "tp"), None, None),
            P(("sp", "tp"), None, None),
        ),
        out_specs=P(("sp", "tp"), None),
        check_vma=False,
    )
```

```python
import functools
import math

import jax
import jax.numpy as jnp
from jax import lax
from jax.experimental import pallas as pl
from jax.experimental.pallas import tpu as pltpu
from jax.sharding import PartitionSpec as P

HEAD_DIM = 64


NORM_EPS = 1e-06
MASKED = -1e30
LOG2E = math.log2(math.e)
MESH = pl.DeviceIdType.MESH
TILE = 256
QROWS = 256
SLOTS = 3
GROUP = 32


def rms_scale(rows, gain):
    mean_sq = jnp.mean(rows * rows, axis=-1, keepdims=True)
    return rows * lax.rsqrt(mean_sq + NORM_EPS) * gain


def split3(values):
    first = values.astype(jnp.bfloat16).astype(jnp.float32)
    second = (values - first).astype(jnp.bfloat16).astype(jnp.float32)
    third = (values - first - second).astype(jnp.bfloat16).astype(jnp.float32)
    return first, second, third


def where(sp, tp):
    return dict(device_id=(sp, tp), device_id_type=MESH)


def offset_of(place):
    low, mid, high = place % 4, (place // 4) % 4, (place // 16) % 4
    return low, (mid + low) % 4, (high + mid + low) % 4, place // 64


def layer_kernel(
    q_raw, k_raw, v_raw, gate_ref, ids_ref, residual_ref, mix_ref, pre_ref, post_ref, weight_ref, ow_hbm, wg_hbm, wu_hbm, wd_hbm, out_ref,
    q_ref, kv_ref, tables, scalars, q_in, q_use, kv_buf, gate_cols, k_aug, s_buf, v_one, gate_buf, peak, acc, o_out, o_in, att,
    ow, wg, wu, wd, slab_wide, slab, stream, outgoing, arrived_rows, results, returned,
    x_wide, x_rows, y_wide,
    kv_send, kv_recv, fwd_send, fwd_recv, q_send, q_recv, gate_send, gate_recv, o_send, o_recv,
    table_sem, w_sem, go_send, go_recv, back_send, back_recv,
):
    tok = k_raw.shape[0]
    half = tok // 2
    sp, tp = lax.axis_index("sp"), lax.axis_index("tp")
    z, x = sp // 4, sp % 4
    y, core = tp // 2, tp % 2
    partner = 2 * y + (1 - core)
    bz, bx = z // 2, x // 2
    zl, xl = jnp.minimum(z, 3 - z), jnp.minimum(x, 3 - x)
    zh, xh = 3 - zl, 3 - xl
    top_block = 4 * zh + xh
    pair_of_me = jnp.abs(bz - bx)
    owner = core == bz
    low_block = 4 * zl + jnp.where(core == 0, xl, xh)
    blocks = (low_block, 15 - low_block)

    def copy(src, dst, send_sem, recv_sem, dev_sp, dev_tp):
        return pltpu.make_async_remote_copy(
            src_ref=src, dst_ref=dst, send_sem=send_sem, recv_sem=recv_sem, **where(dev_sp, dev_tp)
        )

    loads = [
        pltpu.make_async_copy(src, dst, w_sem.at[i])
        for i, (src, dst) in enumerate(((ow_hbm, ow), (wg_hbm, wg), (wu_hbm, wu), (wd_hbm, wd)))
    ]
    for load in loads:
        load.start()

    def peer(place, sign):
        dz, dx, dy, dcore = offset_of(place)
        return (
            4 * ((z + sign * dz + 4) % 4) + (x + sign * dx + 4) % 4,
            2 * ((y + sign * dy + 4) % 4) + (core + dcore) % 2,
        )

    barrier = pltpu.get_barrier_semaphore()

    for d_tp in range(8):
        other_tp = (tp + d_tp) % 8
        for d_sp in range(16):
            if d_sp + d_tp > 0:
                pl.semaphore_signal(barrier, inc=1, **where((sp + d_sp) % 16, other_tp))

    for r in range(0, tok, QROWS):
        rows = slice(r, r + QROWS)
        left = lax.broadcasted_iota(jnp.int32, (QROWS, 128), 1) < HEAD_DIM
        keys, values = k_raw[rows, :].astype(jnp.float32), v_raw[rows, :].astype(jnp.float32)
        kv_ref[0, rows, :] = jnp.where(left, keys, pltpu.roll(values, 64, 1)).astype(jnp.bfloat16)
        kv_ref[1, rows, :] = jnp.where(left, pltpu.roll(keys, 64, 1), values).astype(jnp.bfloat16)
        if r < half:
            top = q_raw[rows, :].astype(jnp.float32)
            low = q_raw[half + r:half + r + QROWS, :].astype(jnp.float32)
            q_ref[0, rows, :] = jnp.where(left, top, pltpu.roll(low, 64, 1)).astype(jnp.bfloat16)
            q_ref[1, rows, :] = jnp.where(left, pltpu.roll(top, 64, 1), low).astype(jnp.bfloat16)

    pl.semaphore_wait(barrier, 127)

    q_copies = []
    for side in range(2):
        dest_sp = 4 * jnp.where(core == 0, zl, zh) + (xl if side == 0 else xh)
        dest_tp = 2 * y + pair_of_me
        mine = (dest_sp == sp) & (dest_tp == tp)
        cp = copy(q_ref.at[side], q_in.at[bz], q_send.at[side], q_recv.at[bz], dest_sp, dest_tp)
        q_copies.append((mine, cp))

        @pl.when(jnp.logical_not(mine))
        def _():
            cp.start()

        @pl.when(mine)
        def _():
            q_in[bz] = q_ref[side]

    gate_cp = copy(gate_ref, gate_buf, gate_send, gate_recv, sp, partner)
    own_cp = copy(kv_ref.at[bx], kv_buf.at[0], fwd_send.at[0], fwd_recv.at[0], sp, partner)

    @pl.when(owner)
    def _():
        gate_cp.start()
        own_cp.start()
        gate_buf[...] = gate_ref[...]
        kv_buf[0] = kv_ref[bx]

    def step_offset(k):
        return (-1369213168 >> (2 * k)) & 3, (-1182141244 >> (2 * k)) & 3

    def kv_out(k, d):
        dz, dx = step_offset(k)
        dest_z, dest_x = (z - dz + 4) % 4, (x - dx + 4) % 4
        top = 4 * jnp.maximum(dest_z, 3 - dest_z) + jnp.maximum(dest_x, 3 - dest_x)
        used = (dest_z // 2 == core) & (sp <= top)
        rows = pl.ds(d * half, half)
        return used, copy(
            kv_ref.at[dest_x // 2, rows], kv_buf.at[k, rows], kv_send.at[k, d], kv_recv.at[k],
            4 * dest_z + dest_x, 2 * y + d,
        )

    def source(k):
        dz, dx = step_offset(k)
        return 4 * ((z + dz) % 4) + (x + dx) % 4

    def send_kv(k, carry):
        for d in range(2):
            used, cp = kv_out(k, d)

            @pl.when(used)
            def _():
                cp.start()

        return carry

    lax.fori_loop(1, 9, send_kv, 0)

    at_sub = lax.broadcasted_iota(jnp.int32, (128, 128), 0)
    at_lane = lax.broadcasted_iota(jnp.int32, (128, 128), 1)
    rows_of = [ids_ref[e:e + 1, :] for e in range(2)]
    columns_of = [jnp.sum(jnp.where(at_sub == at_lane, r, 0), axis=1, keepdims=True) for r in rows_of]
    spots = []
    for ids in rows_of:
        earlier = jnp.zeros((128, 128), jnp.int32)
        for c in columns_of:
            earlier = earlier + jnp.where((c == ids) & (at_sub < at_lane), 1, 0)
        rank = jnp.sum(earlier, axis=0, keepdims=True)
        dz = ((ids >> 5) - z + 4) & 3
        dx = ((ids >> 3) - x + 4) & 3
        dy = ((ids >> 1) - y + 4) & 3
        dcore = (ids + core) & 1
        mid = (dx - dz + 4) & 3
        high = (dy - dz - mid + 8) & 3
        spot = (dz + 4 * mid + 16 * high + 64 * dcore) * SLOTS + rank
        spots.append(jnp.minimum(spot, 128 * SLOTS - 1))
    slot_row = lax.broadcasted_iota(jnp.int32, (128, 128 * SLOTS), 1)
    slot_sub = lax.broadcasted_iota(jnp.int32, (128, 128 * SLOTS), 0)
    token = jnp.zeros((128, 128 * SLOTS), jnp.int32)
    for spot in spots:
        column = jnp.sum(jnp.where(at_sub == at_lane, spot, 0), axis=1, keepdims=True)
        token = token + jnp.where(column == slot_row, slot_sub, 0)
    tables[0:1, :] = jnp.minimum(jnp.sum(token, axis=0, keepdims=True), 127)
    tables[1:2, 0:128] = spots[0]
    tables[2:3, 0:128] = spots[1]
    table_copy = pltpu.make_async_copy(tables, scalars, table_sem)
    table_copy.start()

    def arrived(k):
        rows = pl.ds(core * half, half)
        return copy(kv_buf.at[k, rows], kv_buf.at[k, rows], kv_send.at[0, 0], kv_recv.at[k], sp, partner)

    def passed(k):
        rows = pl.ds(core * half, half)
        return copy(kv_buf.at[k, rows], kv_buf.at[k, rows], fwd_send.at[k], fwd_recv.at[k], sp, partner)

    def expected(k):
        rows = pl.ds((1 - core) * half, half)
        return copy(kv_buf.at[k, rows], kv_buf.at[k, rows], fwd_send.at[k], fwd_recv.at[k], sp, partner)

    @pl.when(jnp.logical_not(owner))
    def _():
        gate_cp.wait_recv()

    peak[...] = jnp.full_like(peak, MASKED)
    acc[...] = jnp.zeros_like(acc)
    lane = lax.broadcasted_iota(jnp.int32, (QROWS, 128), 1)
    at_row = lax.broadcasted_iota(jnp.int32, (8, 128), 0)
    at_lane = lax.broadcasted_iota(jnp.int32, (8, 128), 1)
    put = jnp.where(
        (at_lane == at_row + HEAD_DIM) & (at_row < 3) | (at_row == 3) & (at_lane >= HEAD_DIM + 3) & (at_lane < HEAD_DIM + 6),
        1.0, 0.0,
    ).astype(jnp.bfloat16)
    row8 = lax.broadcasted_iota(jnp.int32, (8, tok), 0)

    def gate_row(j):
        span = pl.ds(pl.multiple_of(j * tok, tok), tok)
        return jnp.where(bx == 0, gate_buf[0:1, span], gate_buf[1:2, span])

    def columns(j, carry):
        parts = split3(gate_row(j) * -LOG2E)
        stack = jnp.where(row8 == 3, 1.0, 0.0)
        for i in range(3):
            stack = jnp.where(row8 == i, parts[i], stack)
        gate_cols[j] = lax.dot_general(
            stack.astype(jnp.bfloat16), put, (((0,), (0,)), ((), ())), preferred_element_type=jnp.float32
        ).astype(jnp.bfloat16)
        return carry

    lax.fori_loop(0, 16, columns, 0)
    for slot in range(2):
        from_x = jnp.where(core == slot, xl, xh)
        from_sp = 4 * (zl if slot == 0 else zh) + from_x
        local = (from_sp == sp) & owner

        @pl.when(jnp.logical_not(local))
        def _():
            copy(q_ref.at[0], q_in.at[slot], q_send.at[0], q_recv.at[slot], sp, partner).wait_recv()

        base = gate_row(blocks[slot])[:, 0:1] * LOG2E
        pieces = split3(base)
        for r in range(tok // QROWS):
            rows = pl.ds(r * QROWS, QROWS)
            wide = q_in[slot, pl.ds(r * QROWS % half, QROWS), :].astype(jnp.float32) * (LOG2E * HEAD_DIM ** -0.5)
            wide = wide if r * QROWS < half else pltpu.roll(wide, 64, 1)
            high = jnp.where(lane < HEAD_DIM, wide, 0.0).astype(jnp.bfloat16)
            low = (wide - high.astype(jnp.float32)).astype(jnp.bfloat16).astype(jnp.float32)
            extra = jnp.where(lane < HEAD_DIM + 3, 1.0, 0.0)
            for i in range(3):
                extra = jnp.where(lane == HEAD_DIM + 3 + i, pieces[i], extra)
            q_use[slot, rows, 0:128] = high
            q_use[slot, rows, 128:256] = jnp.where(lane < HEAD_DIM, low, extra).astype(jnp.bfloat16)

    @pl.when(jnp.logical_not(owner))
    def _():
        own_cp.wait_recv()

    def attend(slot, diagonal):
        tiles = tok // TILE
        keys = [(r + 1) * TILE if diagonal else tok for r in range(tiles)]
        olds, news = [], []
        for i in range(tiles + 1):
            if i < tiles:
                rows = slice(i * TILE, (i + 1) * TILE)
                s = lax.dot_general(
                    q_use[slot, rows, :], k_aug[0:keys[i], :], (((1,), (1,)), ((), ())),
                    preferred_element_type=jnp.float32,
                )
                if diagonal:
                    q_pos = lax.broadcasted_iota(jnp.int32, (TILE, TILE), 0)
                    k_pos = lax.broadcasted_iota(jnp.int32, (TILE, TILE), 1)
                    last = jnp.where(k_pos <= q_pos, s[:, keys[i] - TILE:], MASKED)
                    s = last if i == 0 else jnp.concatenate([s[:, :keys[i] - TILE], last], axis=1)
                s_buf[i % s_buf.shape[0], :, 0:keys[i]] = s
                olds.append(peak[slot, rows, :])
                news.append(jnp.maximum(olds[i], jnp.max(s, axis=1, keepdims=True)))
                peak[slot, rows, :] = news[i]
            if i > 0:
                r = i - 1
                rows = slice(r * TILE, (r + 1) * TILE)
                p = jnp.exp2(s_buf[r % s_buf.shape[0], :, 0:keys[r]] - news[r][:, 0:1]).astype(jnp.bfloat16)
                acc[slot, rows, :] = acc[slot, rows, :] * jnp.exp2(olds[r] - news[r]) + jnp.dot(
                    p, v_one[0:keys[r], :], preferred_element_type=jnp.float32
                )

    def step(k, carry):
        @pl.when(k < 7)
        def _():
            send_kv(k + 9, 0)

        j = source(k)
        follow = source(jnp.minimum(k + 1, 15))
        used = j <= top_block

        @pl.when((k < 15) & (follow <= top_block))
        def _():
            arrived(k + 1).wait_recv()
            passed(k + 1).start()

        @pl.when((k > 0) & used)
        def _():
            expected(k).wait_recv()

        @pl.when(used)
        def _():
            left = lax.broadcasted_iota(jnp.int32, (tok, 128), 1) < HEAD_DIM
            rows_kv = kv_buf[k]
            v_one[...] = jnp.where(left, jnp.bfloat16(1.0), rows_kv)
            k_aug[:, 0:128] = rows_kv
            k_aug[:, 128:256] = jnp.where(left, rows_kv, gate_cols[j])

        for slot in range(2):
            @pl.when(j < blocks[slot])
            def _():
                attend(slot, False)

            @pl.when(j == blocks[slot])
            def _():
                attend(slot, True)

        return carry

    lax.fori_loop(0, 16, step, 0)

    lane64 = lax.broadcasted_iota(jnp.int32, (64, 128), 1)
    head = 4 * y + 2 * bz + bx

    def o_copy(slot, t):
        return copy(o_out.at[slot, t], o_in.at[head], o_send.at[slot, t], o_recv.at[head], blocks[slot], t)

    pieces_out = [(slot, t) for slot in range(2) for t in range(8)]

    def start_o(slot, t):
        mine = (blocks[slot] == sp) & (tp == t)

        @pl.when(mine)
        def _():
            o_in[head] = o_out[slot, t]

        @pl.when(jnp.logical_not(mine))
        def _():
            o_copy(slot, t).start()

    for i, (slot, t) in enumerate(pieces_out):
        o = acc[slot, t * 128:(t + 1) * 128, :]
        o = o / pltpu.roll(o, 64, 1)
        o_out[slot, t] = jnp.where(lane64 < 64, pltpu.roll(o[0:64], 64, 1), o[64:128]).astype(jnp.bfloat16)
        if i % 4 == 3 and i > 3:
            for piece in pieces_out[i - 7:i - 3]:
                start_o(*piece)
    for piece in pieces_out[12:]:
        start_o(*piece)

    for h in range(16):
        r = h % 4
        from_z = zl if r < 2 else zh
        from_x = xl if r % 2 == 0 else xh
        mine = (4 * from_z + from_x == sp) & (2 * (h // 4) + pair_of_me == tp)

        @pl.when(jnp.logical_not(mine))
        def _():
            copy(o_out.at[0, 0], o_in.at[h], o_send.at[0, 0], o_recv.at[h], sp, partner).wait_recv()

    for h in range(0, 16, 2):
        a = o_in[h].astype(jnp.float32)
        b = o_in[h + 1].astype(jnp.float32)
        cols = slice(h * 64, h * 64 + 128)
        att[0:64, cols] = jnp.where(lane64 < 64, a, pltpu.roll(b, 64, 1)).astype(jnp.bfloat16)
        att[64:128, cols] = jnp.where(lane64 < 64, pltpu.roll(a, 64, 1), b).astype(jnp.bfloat16)

    loads[0].wait()
    projected = jnp.dot(att[...], ow[...], preferred_element_type=jnp.float32)
    rows_in = residual_ref[...].astype(jnp.float32) + rms_scale(projected, mix_ref[...])
    rows_in = rows_in.astype(jnp.bfloat16).astype(jnp.float32)
    stream[...] = rows_in
    normed = rms_scale(rows_in, pre_ref[...])
    for c in range(16):
        slab_wide[pl.ds(c, 128, stride=16), :] = normed[:, c * 128:(c + 1) * 128]
    slab[...] = slab_wide[...].reshape(128, 16, 128).astype(jnp.bfloat16)

    def go(place):
        rows = pl.ds(place * SLOTS, SLOTS)
        return copy(
            outgoing.at[rows], arrived_rows.at[rows], go_send, go_recv.at[place // GROUP], *peer(place, 1)
        )

    def back(place):
        rows = pl.ds(place * SLOTS, SLOTS)
        return copy(
            results.at[rows], returned.at[rows], back_send, back_recv.at[place // GROUP], *peer(place, -1)
        )

    def fill(place, carry):
        for s in range(SLOTS):
            outgoing[place * SLOTS + s] = slab[scalars[0, place * SLOTS + s]]
        return carry

    def start_go(place, carry):
        go(place).start()
        return carry

    table_copy.wait()
    for first in range(0, 128 + 16, 16):
        if first < 128:
            lax.fori_loop(first, first + 16, fill, 0, unroll=4)
        if first > 0:
            lax.fori_loop(max(1, first - 16), first, start_go, 0)
    arrived_rows[0:SLOTS] = outgoing[0:SLOTS]
    for load in loads[1:]:
        load.wait()

    def group_rows(group):
        first = SLOTS if group == 0 else group * GROUP * SLOTS
        return pl.ds(first, (group + 1) * GROUP * SLOTS - first)

    def expert_group(group):
        rows = group_rows(group)
        copy(
            outgoing.at[rows], arrived_rows.at[rows], go_send, go_recv.at[group], sp, partner
        ).wait_recv()
        count = GROUP * SLOTS
        first = group * count
        x_wide[...] = arrived_rows[first:first + count].reshape(count * 16, 128).astype(jnp.float32)
        for c in range(16):
            x_rows[:, c * 128:(c + 1) * 128] = x_wide[pl.ds(c, count, stride=16), :].astype(jnp.bfloat16)
        gate_act = jnp.dot(x_rows[...], wg[...], preferred_element_type=jnp.float32)
        up_act = jnp.dot(x_rows[...], wu[...], preferred_element_type=jnp.float32)
        hidden = (gate_act / (1.0 + jnp.exp(-gate_act)) * up_act).astype(jnp.bfloat16)
        y = jnp.dot(hidden, wd[...], preferred_element_type=jnp.float32)
        for c in range(16):
            y_wide[pl.ds(c, count, stride=16), :] = y[:, c * 128:(c + 1) * 128]
        results[first:first + count] = y_wide[...].reshape(count, 16, 128).astype(jnp.bfloat16)

        def start_back(place, carry):
            back(place).start()
            return carry

        lax.fori_loop(max(1, group * GROUP), (group + 1) * GROUP, start_back, 0)
        if group == 0:
            returned[0:SLOTS] = results[0:SLOTS]

    for group in range(128 // GROUP):
        expert_group(group)
    for group in range(128 // GROUP):
        rows = group_rows(group)
        copy(
            results.at[rows], returned.at[rows], back_send, back_recv.at[group], sp, partner
        ).wait_recv()

    def combine(n, carry):
        first = returned[scalars[1, n]].astype(jnp.float32) * weight_ref[0, n]
        second = returned[scalars[2, n]].astype(jnp.float32) * weight_ref[1, n]
        slab_wide[pl.ds(pl.multiple_of(n * 16, 16), 16), :] = first + second
        return carry

    lax.fori_loop(0, 128, combine, 0, unroll=4)
    combined = jnp.concatenate(
        [slab_wide[pl.ds(c, 128, stride=16), :] for c in range(16)], axis=1
    )
    out_ref[...] = (stream[...] + rms_scale(combined, post_ref[...])).astype(jnp.bfloat16)

    for mine, cp in q_copies:
        @pl.when(jnp.logical_not(mine))
        def _():
            cp.wait_send()

    @pl.when(owner)
    def _():
        gate_cp.wait_send()
        own_cp.wait_send()

    def drain(k, carry):
        for d in range(2):
            used, cp = kv_out(k, d)

            @pl.when(used)
            def _():
                cp.wait_send()

        @pl.when(source(k) <= top_block)
        def _():
            passed(k).wait_send()

        return carry

    lax.fori_loop(1, 16, drain, 0)
    for slot in range(2):
        for t in range(8):
            @pl.when(jnp.logical_not((blocks[slot] == sp) & (tp == t)))
            def _():
                o_copy(slot, t).wait_send()
    everything = pl.ds(SLOTS, 127 * SLOTS)
    copy(outgoing.at[everything], arrived_rows.at[everything], go_send, go_recv.at[0], sp, partner).wait_send()
    copy(results.at[everything], returned.at[everything], back_send, back_recv.at[0], sp, partner).wait_send()


def local(
    queries,
    key_rows,
    value_rows,
    cum_gate,
    residual,
    out_weight,
    gain_mix,
    gain_pre,
    gain_post,
    route_ids,
    route_weight,
    w_gate,
    w_up,
    w_down,
):
    tok = queries.shape[0]
    dma = pltpu.SemaphoreType.DMA
    vmem, smem, anywhere = (
        pl.BlockSpec(memory_space=space) for space in (pltpu.VMEM, pltpu.SMEM, pl.ANY)
    )
    bf16, f32 = jnp.bfloat16, jnp.float32
    rows = GROUP * SLOTS
    return pl.pallas_call(
        layer_kernel,
        out_shape=jax.ShapeDtypeStruct((128, 2048), bf16),
        in_specs=[vmem] * 9 + [smem] + [anywhere] * 4,
        out_specs=vmem,
        scratch_shapes=[
            pltpu.VMEM((2, tok // 2, 128), bf16),
            pltpu.VMEM((2, tok, 128), bf16),
            pltpu.VMEM((8, 128 * SLOTS), jnp.int32),
            pltpu.SMEM((8, 128 * SLOTS), jnp.int32),
            pltpu.VMEM((2, tok // 2, 128), bf16),
            pltpu.VMEM((2, tok, 256), bf16),
            pltpu.VMEM((16, tok, 128), jnp.bfloat16),
            pltpu.VMEM((16, tok, 128), jnp.bfloat16),
            pltpu.VMEM((tok, 256), jnp.bfloat16),
            pltpu.VMEM((4, TILE, tok), jnp.float32),
            pltpu.VMEM((tok, 128), bf16),
            pltpu.VMEM((2, 16 * tok), f32),
            pltpu.VMEM((2, tok, 128), f32),
            pltpu.VMEM((2, tok, 128), f32),
            pltpu.VMEM((2, 8, 64, 128), bf16),
            pltpu.VMEM((16, 64, 128), bf16),
            pltpu.VMEM((128, 1024), bf16),
            pltpu.VMEM((1024, 2048), bf16),
            pltpu.VMEM((2048, 512), bf16),
            pltpu.VMEM((2048, 512), bf16),
            pltpu.VMEM((512, 2048), bf16),
            pltpu.VMEM((2048, 128), f32),
            pltpu.VMEM((128, 16, 128), bf16),
            pltpu.VMEM((128, 2048), f32),
            pltpu.VMEM((128 * SLOTS, 16, 128), bf16),
            pltpu.VMEM((128 * SLOTS, 16, 128), bf16),
            pltpu.VMEM((128 * SLOTS, 16, 128), bf16),
            pltpu.VMEM((128 * SLOTS, 16, 128), bf16),
            pltpu.VMEM((rows * 16, 128), f32),
            pltpu.VMEM((rows, 2048), bf16),
            pltpu.VMEM((rows * 16, 128), f32),
            dma((16, 2)), dma((16,)), dma((16,)), dma((16,)), dma((2,)), dma((2,)), dma, dma,
            dma((2, 8)), dma((16,)),
            dma, dma((4,)), dma, dma((128 // GROUP,)), dma, dma((128 // GROUP,)),
        ],
        compiler_params=pltpu.CompilerParams(collective_id=0, has_side_effects=True, vmem_limit_bytes=60 * 1024 * 1024),
        name="layer",
    )(
        queries, key_rows, value_rows, cum_gate, route_ids.T, residual, gain_mix.reshape(1, -1),
        gain_pre.reshape(1, -1), gain_post.reshape(1, -1), route_weight.T,
        out_weight, w_gate[0], w_up[0], w_down[0],
    )


def solution(mesh):
    return jax.shard_map(
        local,
        mesh=mesh,
        in_specs=(
            P("sp", "tp"),
            P("sp", "tp"),
            P("sp", "tp"),
            P("tp", None),
            P(("sp", "tp"), None),
            P(),
            P(),
            P(),
            P(),
            P(("sp", "tp"), None),
            P(("sp", "tp"), None),
            P(("sp", "tp"), None, None),
            P(("sp", "tp"), None, None),
            P(("sp", "tp"), None, None),
        ),
        out_specs=P(("sp", "tp"), None),
        check_vma=False,
    )
```

```python
import functools
import math

import jax
import jax.numpy as jnp
from jax import lax
from jax.experimental import pallas as pl
from jax.experimental.pallas import tpu as pltpu
from jax.sharding import PartitionSpec as P

HEAD_DIM = 64


NORM_EPS = 1e-06
MASKED = -1e30
LOG2E = math.log2(math.e)
MESH = pl.DeviceIdType.MESH
TILE = 256
QROWS = 256
SLOTS = 3
GROUP = 64


def rms_scale(rows, gain):
    mean_sq = jnp.mean(rows * rows, axis=-1, keepdims=True)
    return rows * lax.rsqrt(mean_sq + NORM_EPS) * gain


def split3(values):
    first = values.astype(jnp.bfloat16).astype(jnp.float32)
    second = (values - first).astype(jnp.bfloat16).astype(jnp.float32)
    third = (values - first - second).astype(jnp.bfloat16).astype(jnp.float32)
    return first, second, third


def where(sp, tp):
    return dict(device_id=(sp, tp), device_id_type=MESH)


def offset_of(place):
    low, mid, high = place % 4, (place // 4) % 4, (place // 16) % 4
    return low, (mid + low) % 4, (high + mid + low) % 4, place // 64


def layer_kernel(
    q_raw, k_raw, v_raw, gate_ref, ids_ref, residual_ref, mix_ref, pre_ref, post_ref, weight_ref, ow_hbm, wg_hbm, wu_hbm, wd_hbm, out_ref,
    q_ref, kv_ref, tables, scalars, q_in, q_use, kv_buf, gate_cols, k_aug, s_buf, v_one, gate_buf, peak, acc, o_out, o_in, att,
    ow, wg, wu, wd, slab_wide, slab, stream, outgoing, arrived_rows, results, returned,
    x_wide, x_rows, y_wide,
    kv_send, kv_recv, fwd_send, fwd_recv, q_send, q_recv, gate_send, gate_recv, o_send, o_recv,
    table_sem, w_sem, go_send, go_recv, back_send, back_recv,
):
    tok = k_raw.shape[0]
    half = tok // 2
    sp, tp = lax.axis_index("sp"), lax.axis_index("tp")
    z, x = sp // 4, sp % 4
    y, core = tp // 2, tp % 2
    partner = 2 * y + (1 - core)
    bz, bx = z // 2, x // 2
    zl, xl = jnp.minimum(z, 3 - z), jnp.minimum(x, 3 - x)
    zh, xh = 3 - zl, 3 - xl
    top_block = 4 * zh + xh
    pair_of_me = jnp.abs(bz - bx)
    owner = core == bz
    low_block = 4 * zl + jnp.where(core == 0, xl, xh)
    blocks = (low_block, 15 - low_block)

    def copy(src, dst, send_sem, recv_sem, dev_sp, dev_tp):
        return pltpu.make_async_remote_copy(
            src_ref=src, dst_ref=dst, send_sem=send_sem, recv_sem=recv_sem, **where(dev_sp, dev_tp)
        )

    loads = [
        pltpu.make_async_copy(src, dst, w_sem.at[i])
        for i, (src, dst) in enumerate(((ow_hbm, ow), (wg_hbm, wg), (wu_hbm, wu), (wd_hbm, wd)))
    ]
    for load in loads:
        load.start()

    def peer(place, sign):
        dz, dx, dy, dcore = offset_of(place)
        return (
            4 * ((z + sign * dz + 4) % 4) + (x + sign * dx + 4) % 4,
            2 * ((y + sign * dy + 4) % 4) + (core + dcore) % 2,
        )

    barrier = pltpu.get_barrier_semaphore()

    for d_tp in range(8):
        other_tp = (tp + d_tp) % 8
        for d_sp in range(16):
            if d_sp + d_tp > 0:
                pl.semaphore_signal(barrier, inc=1, **where((sp + d_sp) % 16, other_tp))

    for r in range(0, tok, QROWS):
        rows = slice(r, r + QROWS)
        left = lax.broadcasted_iota(jnp.int32, (QROWS, 128), 1) < HEAD_DIM
        keys, values = k_raw[rows, :].astype(jnp.float32), v_raw[rows, :].astype(jnp.float32)
        kv_ref[0, rows, :] = jnp.where(left, keys, pltpu.roll(values, 64, 1)).astype(jnp.bfloat16)
        kv_ref[1, rows, :] = jnp.where(left, pltpu.roll(keys, 64, 1), values).astype(jnp.bfloat16)
        if r < half:
            top = q_raw[rows, :].astype(jnp.float32)
            low = q_raw[half + r:half + r + QROWS, :].astype(jnp.float32)
            q_ref[0, rows, :] = jnp.where(left, top, pltpu.roll(low, 64, 1)).astype(jnp.bfloat16)
            q_ref[1, rows, :] = jnp.where(left, pltpu.roll(top, 64, 1), low).astype(jnp.bfloat16)

    pl.semaphore_wait(barrier, 127)

    q_copies = []
    for side in range(2):
        dest_sp = 4 * jnp.where(core == 0, zl, zh) + (xl if side == 0 else xh)
        dest_tp = 2 * y + pair_of_me
        mine = (dest_sp == sp) & (dest_tp == tp)
        cp = copy(q_ref.at[side], q_in.at[bz], q_send.at[side], q_recv.at[bz], dest_sp, dest_tp)
        q_copies.append((mine, cp))

        @pl.when(jnp.logical_not(mine))
        def _():
            cp.start()

        @pl.when(mine)
        def _():
            q_in[bz] = q_ref[side]

    gate_cp = copy(gate_ref, gate_buf, gate_send, gate_recv, sp, partner)
    own_cp = copy(kv_ref.at[bx], kv_buf.at[0], fwd_send.at[0], fwd_recv.at[0], sp, partner)

    @pl.when(owner)
    def _():
        gate_cp.start()
        own_cp.start()
        gate_buf[...] = gate_ref[...]
        kv_buf[0] = kv_ref[bx]

    def step_offset(k):
        return (-1369213168 >> (2 * k)) & 3, (-1182141244 >> (2 * k)) & 3

    def kv_out(k, d):
        dz, dx = step_offset(k)
        dest_z, dest_x = (z - dz + 4) % 4, (x - dx + 4) % 4
        top = 4 * jnp.maximum(dest_z, 3 - dest_z) + jnp.maximum(dest_x, 3 - dest_x)
        used = (dest_z // 2 == core) & (sp <= top)
        rows = pl.ds(d * half, half)
        return used, copy(
            kv_ref.at[dest_x // 2, rows], kv_buf.at[k, rows], kv_send.at[k, d], kv_recv.at[k],
            4 * dest_z + dest_x, 2 * y + d,
        )

    def source(k):
        dz, dx = step_offset(k)
        return 4 * ((z + dz) % 4) + (x + dx) % 4

    def send_kv(k, carry):
        for d in range(2):
            used, cp = kv_out(k, d)

            @pl.when(used)
            def _():
                cp.start()

        return carry

    lax.fori_loop(1, 9, send_kv, 0)

    at_sub = lax.broadcasted_iota(jnp.int32, (128, 128), 0)
    at_lane = lax.broadcasted_iota(jnp.int32, (128, 128), 1)
    rows_of = [ids_ref[e:e + 1, :] for e in range(2)]
    columns_of = [jnp.sum(jnp.where(at_sub == at_lane, r, 0), axis=1, keepdims=True) for r in rows_of]
    spots = []
    for ids in rows_of:
        earlier = jnp.zeros((128, 128), jnp.int32)
        for c in columns_of:
            earlier = earlier + jnp.where((c == ids) & (at_sub < at_lane), 1, 0)
        rank = jnp.sum(earlier, axis=0, keepdims=True)
        dz = ((ids >> 5) - z + 4) & 3
        dx = ((ids >> 3) - x + 4) & 3
        dy = ((ids >> 1) - y + 4) & 3
        dcore = (ids + core) & 1
        mid = (dx - dz + 4) & 3
        high = (dy - dz - mid + 8) & 3
        spot = (dz + 4 * mid + 16 * high + 64 * dcore) * SLOTS + rank
        spots.append(jnp.minimum(spot, 128 * SLOTS - 1))
    slot_row = lax.broadcasted_iota(jnp.int32, (128, 128 * SLOTS), 1)
    slot_sub = lax.broadcasted_iota(jnp.int32, (128, 128 * SLOTS), 0)
    token = jnp.zeros((128, 128 * SLOTS), jnp.int32)
    for spot in spots:
        column = jnp.sum(jnp.where(at_sub == at_lane, spot, 0), axis=1, keepdims=True)
        token = token + jnp.where(column == slot_row, slot_sub, 0)
    tables[0:1, :] = jnp.minimum(jnp.sum(token, axis=0, keepdims=True), 127)
    tables[1:2, 0:128] = spots[0]
    tables[2:3, 0:128] = spots[1]
    table_copy = pltpu.make_async_copy(tables, scalars, table_sem)
    table_copy.start()

    def arrived(k):
        rows = pl.ds(core * half, half)
        return copy(kv_buf.at[k, rows], kv_buf.at[k, rows], kv_send.at[0, 0], kv_recv.at[k], sp, partner)

    def passed(k):
        rows = pl.ds(core * half, half)
        return copy(kv_buf.at[k, rows], kv_buf.at[k, rows], fwd_send.at[k], fwd_recv.at[k], sp, partner)

    def expected(k):
        rows = pl.ds((1 - core) * half, half)
        return copy(kv_buf.at[k, rows], kv_buf.at[k, rows], fwd_send.at[k], fwd_recv.at[k], sp, partner)

    @pl.when(jnp.logical_not(owner))
    def _():
        gate_cp.wait_recv()

    peak[...] = jnp.full_like(peak, MASKED)
    acc[...] = jnp.zeros_like(acc)
    lane = lax.broadcasted_iota(jnp.int32, (QROWS, 128), 1)
    at_row = lax.broadcasted_iota(jnp.int32, (8, 128), 0)
    at_lane = lax.broadcasted_iota(jnp.int32, (8, 128), 1)
    put = jnp.where(
        (at_lane == at_row + HEAD_DIM) & (at_row < 3) | (at_row == 3) & (at_lane >= HEAD_DIM + 3) & (at_lane < HEAD_DIM + 6),
        1.0, 0.0,
    ).astype(jnp.bfloat16)
    row8 = lax.broadcasted_iota(jnp.int32, (8, tok), 0)

    def gate_row(j):
        span = pl.ds(pl.multiple_of(j * tok, tok), tok)
        return jnp.where(bx == 0, gate_buf[0:1, span], gate_buf[1:2, span])

    def columns(j, carry):
        parts = split3(gate_row(j) * -LOG2E)
        stack = jnp.where(row8 == 3, 1.0, 0.0)
        for i in range(3):
            stack = jnp.where(row8 == i, parts[i], stack)
        gate_cols[j] = lax.dot_general(
            stack.astype(jnp.bfloat16), put, (((0,), (0,)), ((), ())), preferred_element_type=jnp.float32
        ).astype(jnp.bfloat16)
        return carry

    lax.fori_loop(0, 16, columns, 0, unroll=4)
    for slot in range(2):
        from_x = jnp.where(core == slot, xl, xh)
        from_sp = 4 * (zl if slot == 0 else zh) + from_x
        local = (from_sp == sp) & owner

        @pl.when(jnp.logical_not(local))
        def _():
            copy(q_ref.at[0], q_in.at[slot], q_send.at[0], q_recv.at[slot], sp, partner).wait_recv()

        base = gate_row(blocks[slot])[:, 0:1] * LOG2E
        pieces = split3(base)
        for r in range(tok // QROWS):
            rows = pl.ds(r * QROWS, QROWS)
            wide = q_in[slot, pl.ds(r * QROWS % half, QROWS), :].astype(jnp.float32) * (LOG2E * HEAD_DIM ** -0.5)
            wide = wide if r * QROWS < half else pltpu.roll(wide, 64, 1)
            high = jnp.where(lane < HEAD_DIM, wide, 0.0).astype(jnp.bfloat16)
            low = (wide - high.astype(jnp.float32)).astype(jnp.bfloat16).astype(jnp.float32)
            extra = jnp.where(lane < HEAD_DIM + 3, 1.0, 0.0)
            for i in range(3):
                extra = jnp.where(lane == HEAD_DIM + 3 + i, pieces[i], extra)
            q_use[slot, rows, 0:128] = high
            q_use[slot, rows, 128:256] = jnp.where(lane < HEAD_DIM, low, extra).astype(jnp.bfloat16)

    @pl.when(jnp.logical_not(owner))
    def _():
        own_cp.wait_recv()

    def attend(slot, diagonal):
        tiles = tok // TILE
        keys = [(r + 1) * TILE if diagonal else tok for r in range(tiles)]
        olds, news = [], []
        for i in range(tiles + 1):
            if i < tiles:
                rows = slice(i * TILE, (i + 1) * TILE)
                s = lax.dot_general(
                    q_use[slot, rows, :], k_aug[0:keys[i], :], (((1,), (1,)), ((), ())),
                    preferred_element_type=jnp.float32,
                )
                if diagonal:
                    q_pos = lax.broadcasted_iota(jnp.int32, (TILE, TILE), 0)
                    k_pos = lax.broadcasted_iota(jnp.int32, (TILE, TILE), 1)
                    last = jnp.where(k_pos <= q_pos, s[:, keys[i] - TILE:], MASKED)
                    s = last if i == 0 else jnp.concatenate([s[:, :keys[i] - TILE], last], axis=1)
                s_buf[i % s_buf.shape[0], :, 0:keys[i]] = s
                olds.append(peak[slot, rows, :])
                news.append(jnp.maximum(olds[i], jnp.max(s, axis=1, keepdims=True)))
                peak[slot, rows, :] = news[i]
            if i > 0:
                r = i - 1
                rows = slice(r * TILE, (r + 1) * TILE)
                p = jnp.exp2(s_buf[r % s_buf.shape[0], :, 0:keys[r]] - news[r][:, 0:1]).astype(jnp.bfloat16)
                acc[slot, rows, :] = acc[slot, rows, :] * jnp.exp2(olds[r] - news[r]) + jnp.dot(
                    p, v_one[0:keys[r], :], preferred_element_type=jnp.float32
                )

    def step(k, carry):
        @pl.when(k < 7)
        def _():
            send_kv(k + 9, 0)

        j = source(k)
        follow = source(jnp.minimum(k + 1, 15))
        used = j <= top_block

        @pl.when((k < 15) & (follow <= top_block))
        def _():
            arrived(k + 1).wait_recv()
            passed(k + 1).start()

        @pl.when((k > 0) & used)
        def _():
            expected(k).wait_recv()

        @pl.when(used)
        def _():
            left = lax.broadcasted_iota(jnp.int32, (tok, 128), 1) < HEAD_DIM
            rows_kv = kv_buf[k]
            v_one[...] = jnp.where(left, jnp.bfloat16(1.0), rows_kv)
            k_aug[:, 0:128] = rows_kv
            k_aug[:, 128:256] = jnp.where(left, rows_kv, gate_cols[j])

        for slot in range(2):
            @pl.when(j < blocks[slot])
            def _():
                attend(slot, False)

            @pl.when(j == blocks[slot])
            def _():
                attend(slot, True)

        return carry

    lax.fori_loop(0, 16, step, 0)

    lane64 = lax.broadcasted_iota(jnp.int32, (64, 128), 1)
    head = 4 * y + 2 * bz + bx

    def o_copy(slot, t):
        return copy(o_out.at[slot, t], o_in.at[head], o_send.at[slot, t], o_recv.at[head], blocks[slot], t)

    pieces_out = [(slot, t) for slot in range(2) for t in range(8)]

    def start_o(slot, t):
        mine = (blocks[slot] == sp) & (tp == t)

        @pl.when(mine)
        def _():
            o_in[head] = o_out[slot, t]

        @pl.when(jnp.logical_not(mine))
        def _():
            o_copy(slot, t).start()

    for i, (slot, t) in enumerate(pieces_out):
        o = acc[slot, t * 128:(t + 1) * 128, :]
        o = o / pltpu.roll(o, 64, 1)
        o_out[slot, t] = jnp.where(lane64 < 64, pltpu.roll(o[0:64], 64, 1), o[64:128]).astype(jnp.bfloat16)
        if i % 4 == 3 and i > 3:
            for piece in pieces_out[i - 7:i - 3]:
                start_o(*piece)
    for piece in pieces_out[12:]:
        start_o(*piece)

    for h in range(16):
        r = h % 4
        from_z = zl if r < 2 else zh
        from_x = xl if r % 2 == 0 else xh
        mine = (4 * from_z + from_x == sp) & (2 * (h // 4) + pair_of_me == tp)

        @pl.when(jnp.logical_not(mine))
        def _():
            copy(o_out.at[0, 0], o_in.at[h], o_send.at[0, 0], o_recv.at[h], sp, partner).wait_recv()

    for h in range(0, 16, 2):
        a = o_in[h].astype(jnp.float32)
        b = o_in[h + 1].astype(jnp.float32)
        cols = slice(h * 64, h * 64 + 128)
        att[0:64, cols] = jnp.where(lane64 < 64, a, pltpu.roll(b, 64, 1)).astype(jnp.bfloat16)
        att[64:128, cols] = jnp.where(lane64 < 64, pltpu.roll(a, 64, 1), b).astype(jnp.bfloat16)

    loads[0].wait()
    projected = jnp.dot(att[...], ow[...], preferred_element_type=jnp.float32)
    rows_in = residual_ref[...].astype(jnp.float32) + rms_scale(projected, mix_ref[...])
    rows_in = rows_in.astype(jnp.bfloat16).astype(jnp.float32)
    stream[...] = rows_in
    normed = rms_scale(rows_in, pre_ref[...])
    for c in range(16):
        slab_wide[pl.ds(c, 128, stride=16), :] = normed[:, c * 128:(c + 1) * 128]
    slab[...] = slab_wide[...].reshape(128, 16, 128).astype(jnp.bfloat16)

    def go(place):
        rows = pl.ds(place * SLOTS, SLOTS)
        return copy(
            outgoing.at[rows], arrived_rows.at[rows], go_send, go_recv.at[place // GROUP], *peer(place, 1)
        )

    def back(place):
        rows = pl.ds(place * SLOTS, SLOTS)
        return copy(
            results.at[rows], returned.at[rows], back_send, back_recv.at[place // GROUP], *peer(place, -1)
        )

    def fill(place, carry):
        for s in range(SLOTS):
            outgoing[place * SLOTS + s] = slab[scalars[0, place * SLOTS + s]]
        return carry

    def start_go(place, carry):
        go(place).start()
        return carry

    table_copy.wait()
    for first in range(0, 128 + 16, 16):
        if first < 128:
            lax.fori_loop(first, first + 16, fill, 0, unroll=4)
        if first > 0:
            lax.fori_loop(max(1, first - 16), first, start_go, 0)
    arrived_rows[0:SLOTS] = outgoing[0:SLOTS]
    for load in loads[1:]:
        load.wait()

    def group_rows(group):
        first = SLOTS if group == 0 else group * GROUP * SLOTS
        return pl.ds(first, (group + 1) * GROUP * SLOTS - first)

    def expert_group(group):
        rows = group_rows(group)
        copy(
            outgoing.at[rows], arrived_rows.at[rows], go_send, go_recv.at[group], sp, partner
        ).wait_recv()
        count = GROUP * SLOTS
        first = group * count
        x_wide[...] = arrived_rows[first:first + count].reshape(count * 16, 128).astype(jnp.float32)
        for c in range(16):
            x_rows[:, c * 128:(c + 1) * 128] = x_wide[pl.ds(c, count, stride=16), :].astype(jnp.bfloat16)
        gate_act = jnp.dot(x_rows[...], wg[...], preferred_element_type=jnp.float32)
        up_act = jnp.dot(x_rows[...], wu[...], preferred_element_type=jnp.float32)
        hidden = (gate_act / (1.0 + jnp.exp(-gate_act)) * up_act).astype(jnp.bfloat16)
        y = jnp.dot(hidden, wd[...], preferred_element_type=jnp.float32)
        for c in range(16):
            y_wide[pl.ds(c, count, stride=16), :] = y[:, c * 128:(c + 1) * 128]
        results[first:first + count] = y_wide[...].reshape(count, 16, 128).astype(jnp.bfloat16)

        def start_back(place, carry):
            back(place).start()
            return carry

        lax.fori_loop(max(1, group * GROUP), (group + 1) * GROUP, start_back, 0)
        if group == 0:
            returned[0:SLOTS] = results[0:SLOTS]

    for group in range(128 // GROUP):
        expert_group(group)
    for group in range(128 // GROUP):
        rows = group_rows(group)
        copy(
            results.at[rows], returned.at[rows], back_send, back_recv.at[group], sp, partner
        ).wait_recv()

    def combine(n, carry):
        first = returned[scalars[1, n]].astype(jnp.float32) * weight_ref[0, n]
        second = returned[scalars[2, n]].astype(jnp.float32) * weight_ref[1, n]
        slab_wide[pl.ds(pl.multiple_of(n * 16, 16), 16), :] = first + second
        return carry

    lax.fori_loop(0, 128, combine, 0, unroll=4)
    combined = jnp.concatenate(
        [slab_wide[pl.ds(c, 128, stride=16), :] for c in range(16)], axis=1
    )
    out_ref[...] = (stream[...] + rms_scale(combined, post_ref[...])).astype(jnp.bfloat16)

    for mine, cp in q_copies:
        @pl.when(jnp.logical_not(mine))
        def _():
            cp.wait_send()

    @pl.when(owner)
    def _():
        gate_cp.wait_send()
        own_cp.wait_send()

    def drain(k, carry):
        for d in range(2):
            used, cp = kv_out(k, d)

            @pl.when(used)
            def _():
                cp.wait_send()

        @pl.when(source(k) <= top_block)
        def _():
            passed(k).wait_send()

        return carry

    lax.fori_loop(1, 16, drain, 0)
    for slot in range(2):
        for t in range(8):
            @pl.when(jnp.logical_not((blocks[slot] == sp) & (tp == t)))
            def _():
                o_copy(slot, t).wait_send()
    everything = pl.ds(SLOTS, 127 * SLOTS)
    copy(outgoing.at[everything], arrived_rows.at[everything], go_send, go_recv.at[0], sp, partner).wait_send()
    copy(results.at[everything], returned.at[everything], back_send, back_recv.at[0], sp, partner).wait_send()


def local(
    queries,
    key_rows,
    value_rows,
    cum_gate,
    residual,
    out_weight,
    gain_mix,
    gain_pre,
    gain_post,
    route_ids,
    route_weight,
    w_gate,
    w_up,
    w_down,
):
    tok = queries.shape[0]
    dma = pltpu.SemaphoreType.DMA
    vmem, smem, anywhere = (
        pl.BlockSpec(memory_space=space) for space in (pltpu.VMEM, pltpu.SMEM, pl.ANY)
    )
    bf16, f32 = jnp.bfloat16, jnp.float32
    rows = GROUP * SLOTS
    return pl.pallas_call(
        layer_kernel,
        out_shape=jax.ShapeDtypeStruct((128, 2048), bf16),
        in_specs=[vmem] * 9 + [smem] + [anywhere] * 4,
        out_specs=vmem,
        scratch_shapes=[
            pltpu.VMEM((2, tok // 2, 128), bf16),
            pltpu.VMEM((2, tok, 128), bf16),
            pltpu.VMEM((8, 128 * SLOTS), jnp.int32),
            pltpu.SMEM((8, 128 * SLOTS), jnp.int32),
            pltpu.VMEM((2, tok // 2, 128), bf16),
            pltpu.VMEM((2, tok, 256), bf16),
            pltpu.VMEM((16, tok, 128), jnp.bfloat16),
            pltpu.VMEM((16, tok, 128), jnp.bfloat16),
            pltpu.VMEM((tok, 256), jnp.bfloat16),
            pltpu.VMEM((4, TILE, tok), jnp.float32),
            pltpu.VMEM((tok, 128), bf16),
            pltpu.VMEM((2, 16 * tok), f32),
            pltpu.VMEM((2, tok, 128), f32),
            pltpu.VMEM((2, tok, 128), f32),
            pltpu.VMEM((2, 8, 64, 128), bf16),
            pltpu.VMEM((16, 64, 128), bf16),
            pltpu.VMEM((128, 1024), bf16),
            pltpu.VMEM((1024, 2048), bf16),
            pltpu.VMEM((2048, 512), bf16),
            pltpu.VMEM((2048, 512), bf16),
            pltpu.VMEM((512, 2048), bf16),
            pltpu.VMEM((2048, 128), f32),
            pltpu.VMEM((128, 16, 128), bf16),
            pltpu.VMEM((128, 2048), f32),
            pltpu.VMEM((128 * SLOTS, 16, 128), bf16),
            pltpu.VMEM((128 * SLOTS, 16, 128), bf16),
            pltpu.VMEM((128 * SLOTS, 16, 128), bf16),
            pltpu.VMEM((128 * SLOTS, 16, 128), bf16),
            pltpu.VMEM((rows * 16, 128), f32),
            pltpu.VMEM((rows, 2048), bf16),
            pltpu.VMEM((rows * 16, 128), f32),
            dma((16, 2)), dma((16,)), dma((16,)), dma((16,)), dma((2,)), dma((2,)), dma, dma,
            dma((2, 8)), dma((16,)),
            dma, dma((4,)), dma, dma((128 // GROUP,)), dma, dma((128 // GROUP,)),
        ],
        compiler_params=pltpu.CompilerParams(collective_id=0, has_side_effects=True, vmem_limit_bytes=60 * 1024 * 1024),
        name="layer",
    )(
        queries, key_rows, value_rows, cum_gate, route_ids.T, residual, gain_mix.reshape(1, -1),
        gain_pre.reshape(1, -1), gain_post.reshape(1, -1), route_weight.T,
        out_weight, w_gate[0], w_up[0], w_down[0],
    )


def solution(mesh):
    return jax.shard_map(
        local,
        mesh=mesh,
        in_specs=(
            P("sp", "tp"),
            P("sp", "tp"),
            P("sp", "tp"),
            P("tp", None),
            P(("sp", "tp"), None),
            P(),
            P(),
            P(),
            P(),
            P(("sp", "tp"), None),
            P(("sp", "tp"), None),
            P(("sp", "tp"), None, None),
            P(("sp", "tp"), None, None),
            P(("sp", "tp"), None, None),
        ),
        out_specs=P(("sp", "tp"), None),
        check_vma=False,
    )
```

```python
import functools
import math

import jax
import jax.numpy as jnp
from jax import lax
from jax.experimental import pallas as pl
from jax.experimental.pallas import tpu as pltpu
from jax.sharding import PartitionSpec as P

HEAD_DIM = 64


NORM_EPS = 1e-06
MASKED = -1e30
LOG2E = math.log2(math.e)
MESH = pl.DeviceIdType.MESH
TILE = 256
QROWS = 256
SLOTS = 3
GROUP = 64


def rms_scale(rows, gain):
    mean_sq = jnp.mean(rows * rows, axis=-1, keepdims=True)
    return rows * lax.rsqrt(mean_sq + NORM_EPS) * gain


def split3(values):
    first = values.astype(jnp.bfloat16).astype(jnp.float32)
    second = (values - first).astype(jnp.bfloat16).astype(jnp.float32)
    third = (values - first - second).astype(jnp.bfloat16).astype(jnp.float32)
    return first, second, third


def where(sp, tp):
    return dict(device_id=(sp, tp), device_id_type=MESH)


def offset_of(place):
    low, mid, high = place % 4, (place // 4) % 4, (place // 16) % 4
    return low, (mid + low) % 4, (high + mid + low) % 4, place // 64


def layer_kernel(
    q_raw, k_raw, v_raw, gate_ref, ids_ref, residual_ref, mix_ref, pre_ref, post_ref, weight_ref, ow_hbm, wg_hbm, wu_hbm, wd_hbm, out_ref,
    q_ref, kv_ref, tables, scalars, q_in, q_use, kv_buf, gate_cols, k_aug, s_buf, v_one, gate_buf, peak, acc, o_out, o_in, att,
    ow, wg, wu, wd, slab_wide, slab, stream, outgoing, arrived_rows, results, returned,
    x_wide, x_rows, y_wide,
    kv_send, kv_recv, fwd_send, fwd_recv, q_send, q_recv, gate_send, gate_recv, o_send, o_recv,
    table_sem, w_sem, go_send, go_recv, back_send, back_recv,
):
    tok = k_raw.shape[0]
    half = tok // 2
    sp, tp = lax.axis_index("sp"), lax.axis_index("tp")
    z, x = sp // 4, sp % 4
    y, core = tp // 2, tp % 2
    partner = 2 * y + (1 - core)
    bz, bx = z // 2, x // 2
    zl, xl = jnp.minimum(z, 3 - z), jnp.minimum(x, 3 - x)
    zh, xh = 3 - zl, 3 - xl
    top_block = 4 * zh + xh
    pair_of_me = jnp.abs(bz - bx)
    owner = core == bz
    low_block = 4 * zl + jnp.where(core == 0, xl, xh)
    blocks = (low_block, 15 - low_block)

    def copy(src, dst, send_sem, recv_sem, dev_sp, dev_tp):
        return pltpu.make_async_remote_copy(
            src_ref=src, dst_ref=dst, send_sem=send_sem, recv_sem=recv_sem, **where(dev_sp, dev_tp)
        )

    loads = [
        pltpu.make_async_copy(src, dst, w_sem.at[i])
        for i, (src, dst) in enumerate(((ow_hbm, ow), (wg_hbm, wg), (wu_hbm, wu), (wd_hbm, wd)))
    ]
    for load in loads:
        load.start()

    def peer(place, sign):
        dz, dx, dy, dcore = offset_of(place)
        return (
            4 * ((z + sign * dz + 4) % 4) + (x + sign * dx + 4) % 4,
            2 * ((y + sign * dy + 4) % 4) + (core + dcore) % 2,
        )

    barrier = pltpu.get_barrier_semaphore()

    for d_tp in range(8):
        other_tp = (tp + d_tp) % 8
        for d_sp in range(16):
            if d_sp + d_tp > 0:
                pl.semaphore_signal(barrier, inc=1, **where((sp + d_sp) % 16, other_tp))

    for r in range(0, tok, QROWS):
        rows = slice(r, r + QROWS)
        left = lax.broadcasted_iota(jnp.int32, (QROWS, 128), 1) < HEAD_DIM
        keys, values = k_raw[rows, :].astype(jnp.float32), v_raw[rows, :].astype(jnp.float32)
        kv_ref[0, rows, :] = jnp.where(left, keys, pltpu.roll(values, 64, 1)).astype(jnp.bfloat16)
        kv_ref[1, rows, :] = jnp.where(left, pltpu.roll(keys, 64, 1), values).astype(jnp.bfloat16)
        if r < half:
            top = q_raw[rows, :].astype(jnp.float32)
            low = q_raw[half + r:half + r + QROWS, :].astype(jnp.float32)
            q_ref[0, rows, :] = jnp.where(left, top, pltpu.roll(low, 64, 1)).astype(jnp.bfloat16)
            q_ref[1, rows, :] = jnp.where(left, pltpu.roll(top, 64, 1), low).astype(jnp.bfloat16)

    pl.semaphore_wait(barrier, 127)

    q_copies = []
    for side in range(2):
        dest_sp = 4 * jnp.where(core == 0, zl, zh) + (xl if side == 0 else xh)
        dest_tp = 2 * y + pair_of_me
        mine = (dest_sp == sp) & (dest_tp == tp)
        cp = copy(q_ref.at[side], q_in.at[bz], q_send.at[side], q_recv.at[bz], dest_sp, dest_tp)
        q_copies.append((mine, cp))

        @pl.when(jnp.logical_not(mine))
        def _():
            cp.start()

        @pl.when(mine)
        def _():
            q_in[bz] = q_ref[side]

    gate_cp = copy(gate_ref, gate_buf, gate_send, gate_recv, sp, partner)
    own_cp = copy(kv_ref.at[bx], kv_buf.at[0], fwd_send.at[0], fwd_recv.at[0], sp, partner)

    @pl.when(owner)
    def _():
        gate_cp.start()
        own_cp.start()
        gate_buf[...] = gate_ref[...]
        kv_buf[0] = kv_ref[bx]

    def step_offset(k):
        return (-1369213168 >> (2 * k)) & 3, (-1182141244 >> (2 * k)) & 3

    def kv_out(k, d):
        dz, dx = step_offset(k)
        dest_z, dest_x = (z - dz + 4) % 4, (x - dx + 4) % 4
        top = 4 * jnp.maximum(dest_z, 3 - dest_z) + jnp.maximum(dest_x, 3 - dest_x)
        used = (dest_z // 2 == core) & (sp <= top)
        rows = pl.ds(d * half, half)
        return used, copy(
            kv_ref.at[dest_x // 2, rows], kv_buf.at[k, rows], kv_send.at[k, d], kv_recv.at[k],
            4 * dest_z + dest_x, 2 * y + d,
        )

    def source(k):
        dz, dx = step_offset(k)
        return 4 * ((z + dz) % 4) + (x + dx) % 4

    def send_kv(k, carry):
        for d in range(2):
            used, cp = kv_out(k, d)

            @pl.when(used)
            def _():
                cp.start()

        return carry

    lax.fori_loop(1, 9, send_kv, 0)

    at_sub = lax.broadcasted_iota(jnp.int32, (128, 128), 0)
    at_lane = lax.broadcasted_iota(jnp.int32, (128, 128), 1)
    rows_of = [ids_ref[e:e + 1, :] for e in range(2)]
    columns_of = [jnp.sum(jnp.where(at_sub == at_lane, r, 0), axis=1, keepdims=True) for r in rows_of]
    spots = []
    for ids in rows_of:
        earlier = jnp.zeros((128, 128), jnp.int32)
        for c in columns_of:
            earlier = earlier + jnp.where((c == ids) & (at_sub < at_lane), 1, 0)
        rank = jnp.sum(earlier, axis=0, keepdims=True)
        dz = ((ids >> 5) - z + 4) & 3
        dx = ((ids >> 3) - x + 4) & 3
        dy = ((ids >> 1) - y + 4) & 3
        dcore = (ids + core) & 1
        mid = (dx - dz + 4) & 3
        high = (dy - dz - mid + 8) & 3
        spot = (dz + 4 * mid + 16 * high + 64 * dcore) * SLOTS + rank
        spots.append(jnp.minimum(spot, 128 * SLOTS - 1))
    slot_row = lax.broadcasted_iota(jnp.int32, (128, 128 * SLOTS), 1)
    slot_sub = lax.broadcasted_iota(jnp.int32, (128, 128 * SLOTS), 0)
    token = jnp.zeros((128, 128 * SLOTS), jnp.int32)
    for spot in spots:
        column = jnp.sum(jnp.where(at_sub == at_lane, spot, 0), axis=1, keepdims=True)
        token = token + jnp.where(column == slot_row, slot_sub, 0)
    tables[0:1, :] = jnp.minimum(jnp.sum(token, axis=0, keepdims=True), 127)
    tables[1:2, 0:128] = spots[0]
    tables[2:3, 0:128] = spots[1]
    table_copy = pltpu.make_async_copy(tables, scalars, table_sem)
    table_copy.start()

    def arrived(k):
        rows = pl.ds(core * half, half)
        return copy(kv_buf.at[k, rows], kv_buf.at[k, rows], kv_send.at[0, 0], kv_recv.at[k], sp, partner)

    def passed(k):
        rows = pl.ds(core * half, half)
        return copy(kv_buf.at[k, rows], kv_buf.at[k, rows], fwd_send.at[k], fwd_recv.at[k], sp, partner)

    def expected(k):
        rows = pl.ds((1 - core) * half, half)
        return copy(kv_buf.at[k, rows], kv_buf.at[k, rows], fwd_send.at[k], fwd_recv.at[k], sp, partner)

    @pl.when(jnp.logical_not(owner))
    def _():
        gate_cp.wait_recv()

    peak[...] = jnp.full_like(peak, MASKED)
    acc[...] = jnp.zeros_like(acc)
    lane = lax.broadcasted_iota(jnp.int32, (QROWS, 128), 1)
    at_row = lax.broadcasted_iota(jnp.int32, (8, 128), 0)
    at_lane = lax.broadcasted_iota(jnp.int32, (8, 128), 1)
    put = jnp.where(
        (at_lane == at_row + HEAD_DIM) & (at_row < 3) | (at_row == 3) & (at_lane >= HEAD_DIM + 3) & (at_lane < HEAD_DIM + 6),
        1.0, 0.0,
    ).astype(jnp.bfloat16)
    row8 = lax.broadcasted_iota(jnp.int32, (8, tok), 0)

    def gate_row(j):
        span = pl.ds(pl.multiple_of(j * tok, tok), tok)
        return jnp.where(bx == 0, gate_buf[0:1, span], gate_buf[1:2, span])

    def columns(j, carry):
        parts = split3(gate_row(j) * -LOG2E)
        stack = jnp.where(row8 == 3, 1.0, 0.0)
        for i in range(3):
            stack = jnp.where(row8 == i, parts[i], stack)
        gate_cols[j] = lax.dot_general(
            stack.astype(jnp.bfloat16), put, (((0,), (0,)), ((), ())), preferred_element_type=jnp.float32
        ).astype(jnp.bfloat16)
        return carry

    lax.fori_loop(0, 16, columns, 0, unroll=4)
    for slot in range(2):
        from_x = jnp.where(core == slot, xl, xh)
        from_sp = 4 * (zl if slot == 0 else zh) + from_x
        local = (from_sp == sp) & owner

        @pl.when(jnp.logical_not(local))
        def _():
            copy(q_ref.at[0], q_in.at[slot], q_send.at[0], q_recv.at[slot], sp, partner).wait_recv()

        base = gate_row(blocks[slot])[:, 0:1] * LOG2E
        pieces = split3(base)
        for r in range(tok // QROWS):
            rows = pl.ds(r * QROWS, QROWS)
            wide = q_in[slot, pl.ds(r * QROWS % half, QROWS), :].astype(jnp.float32) * (LOG2E * HEAD_DIM ** -0.5)
            wide = wide if r * QROWS < half else pltpu.roll(wide, 64, 1)
            high = jnp.where(lane < HEAD_DIM, wide, 0.0).astype(jnp.bfloat16)
            low = (wide - high.astype(jnp.float32)).astype(jnp.bfloat16).astype(jnp.float32)
            extra = jnp.where(lane < HEAD_DIM + 3, 1.0, 0.0)
            for i in range(3):
                extra = jnp.where(lane == HEAD_DIM + 3 + i, pieces[i], extra)
            q_use[slot, rows, 0:128] = high
            q_use[slot, rows, 128:256] = jnp.where(lane < HEAD_DIM, low, extra).astype(jnp.bfloat16)

    @pl.when(jnp.logical_not(owner))
    def _():
        own_cp.wait_recv()

    def attend(slot, diagonal):
        tiles = tok // TILE
        keys = [(r + 1) * TILE if diagonal else tok for r in range(tiles)]
        olds, news = [], []
        for i in range(tiles + 1):
            if i < tiles:
                rows = slice(i * TILE, (i + 1) * TILE)
                s = lax.dot_general(
                    q_use[slot, rows, :], k_aug[0:keys[i], :], (((1,), (1,)), ((), ())),
                    preferred_element_type=jnp.float32,
                )
                if diagonal:
                    q_pos = lax.broadcasted_iota(jnp.int32, (TILE, TILE), 0)
                    k_pos = lax.broadcasted_iota(jnp.int32, (TILE, TILE), 1)
                    last = jnp.where(k_pos <= q_pos, s[:, keys[i] - TILE:], MASKED)
                    s = last if i == 0 else jnp.concatenate([s[:, :keys[i] - TILE], last], axis=1)
                s_buf[i % s_buf.shape[0], :, 0:keys[i]] = s
                olds.append(peak[slot, rows, :])
                news.append(jnp.maximum(olds[i], jnp.max(s, axis=1, keepdims=True)))
                peak[slot, rows, :] = news[i]
            if i > 0:
                r = i - 1
                rows = slice(r * TILE, (r + 1) * TILE)
                p = jnp.exp2(s_buf[r % s_buf.shape[0], :, 0:keys[r]] - news[r][:, 0:1]).astype(jnp.bfloat16)
                acc[slot, rows, :] = acc[slot, rows, :] * jnp.exp2(olds[r] - news[r]) + jnp.dot(
                    p, v_one[0:keys[r], :], preferred_element_type=jnp.float32
                )

    def step(k, carry):
        @pl.when(k < 7)
        def _():
            send_kv(k + 9, 0)

        j = source(k)
        follow = source(jnp.minimum(k + 1, 15))
        used = j <= top_block

        @pl.when((k < 15) & (follow <= top_block))
        def _():
            arrived(k + 1).wait_recv()
            passed(k + 1).start()

        @pl.when((k > 0) & used)
        def _():
            expected(k).wait_recv()

        @pl.when(used)
        def _():
            left = lax.broadcasted_iota(jnp.int32, (tok, 128), 1) < HEAD_DIM
            rows_kv = kv_buf[k]
            v_one[...] = jnp.where(left, jnp.bfloat16(1.0), rows_kv)
            k_aug[:, 0:128] = rows_kv
            k_aug[:, 128:256] = jnp.where(left, rows_kv, gate_cols[j])

        for slot in range(2):
            @pl.when(j < blocks[slot])
            def _():
                attend(slot, False)

            @pl.when(j == blocks[slot])
            def _():
                attend(slot, True)

        return carry

    lax.fori_loop(0, 16, step, 0)

    lane64 = lax.broadcasted_iota(jnp.int32, (64, 128), 1)
    head = 4 * y + 2 * bz + bx

    def o_copy(slot, t):
        return copy(o_out.at[slot, t], o_in.at[head], o_send.at[slot, t], o_recv.at[head], blocks[slot], t)

    pieces_out = [(slot, t) for slot in range(2) for t in range(8)]

    def start_o(slot, t):
        mine = (blocks[slot] == sp) & (tp == t)

        @pl.when(mine)
        def _():
            o_in[head] = o_out[slot, t]

        @pl.when(jnp.logical_not(mine))
        def _():
            o_copy(slot, t).start()

    for i, (slot, t) in enumerate(pieces_out):
        o = acc[slot, t * 128:(t + 1) * 128, :]
        o = o / pltpu.roll(o, 64, 1)
        o_out[slot, t] = jnp.where(lane64 < 64, pltpu.roll(o[0:64], 64, 1), o[64:128]).astype(jnp.bfloat16)
        if i % 4 == 3 and i > 3:
            for piece in pieces_out[i - 7:i - 3]:
                start_o(*piece)
    for piece in pieces_out[12:]:
        start_o(*piece)

    for h in range(16):
        r = h % 4
        from_z = zl if r < 2 else zh
        from_x = xl if r % 2 == 0 else xh
        mine = (4 * from_z + from_x == sp) & (2 * (h // 4) + pair_of_me == tp)

        @pl.when(jnp.logical_not(mine))
        def _():
            copy(o_out.at[0, 0], o_in.at[h], o_send.at[0, 0], o_recv.at[h], sp, partner).wait_recv()

    for h in range(0, 16, 2):
        a = o_in[h].astype(jnp.float32)
        b = o_in[h + 1].astype(jnp.float32)
        cols = slice(h * 64, h * 64 + 128)
        att[0:64, cols] = jnp.where(lane64 < 64, a, pltpu.roll(b, 64, 1)).astype(jnp.bfloat16)
        att[64:128, cols] = jnp.where(lane64 < 64, pltpu.roll(a, 64, 1), b).astype(jnp.bfloat16)

    loads[0].wait()
    projected = jnp.dot(att[...], ow[...], preferred_element_type=jnp.float32)
    rows_in = residual_ref[...].astype(jnp.float32) + rms_scale(projected, mix_ref[...])
    rows_in = rows_in.astype(jnp.bfloat16).astype(jnp.float32)
    stream[...] = rows_in
    normed = rms_scale(rows_in, pre_ref[...])
    for c in range(16):
        slab_wide[pl.ds(c, 128, stride=16), :] = normed[:, c * 128:(c + 1) * 128]
    slab[...] = slab_wide[...].reshape(128, 16, 128).astype(jnp.bfloat16)

    def go(place):
        rows = pl.ds(place * SLOTS, SLOTS)
        return copy(
            outgoing.at[rows], arrived_rows.at[rows], go_send, go_recv.at[place // GROUP], *peer(place, 1)
        )

    def back(place):
        rows = pl.ds(place * SLOTS, SLOTS)
        return copy(
            results.at[rows], returned.at[rows], back_send, back_recv.at[place // GROUP], *peer(place, -1)
        )

    def fill(place, carry):
        for s in range(SLOTS):
            outgoing[place * SLOTS + s] = slab[scalars[0, place * SLOTS + s]]
        return carry

    def start_go(place, carry):
        go(place).start()
        return carry

    table_copy.wait()
    for first in range(0, 128 + 16, 16):
        if first < 128:
            lax.fori_loop(first, first + 16, fill, 0, unroll=16)
        if first > 0:
            lax.fori_loop(max(1, first - 16), first, start_go, 0)
    arrived_rows[0:SLOTS] = outgoing[0:SLOTS]
    for load in loads[1:]:
        load.wait()

    def group_rows(group):
        first = SLOTS if group == 0 else group * GROUP * SLOTS
        return pl.ds(first, (group + 1) * GROUP * SLOTS - first)

    def expert_group(group):
        rows = group_rows(group)
        copy(
            outgoing.at[rows], arrived_rows.at[rows], go_send, go_recv.at[group], sp, partner
        ).wait_recv()
        count = GROUP * SLOTS
        first = group * count
        x_wide[...] = arrived_rows[first:first + count].reshape(count * 16, 128).astype(jnp.float32)
        for c in range(16):
            x_rows[:, c * 128:(c + 1) * 128] = x_wide[pl.ds(c, count, stride=16), :].astype(jnp.bfloat16)
        gate_act = jnp.dot(x_rows[...], wg[...], preferred_element_type=jnp.float32)
        up_act = jnp.dot(x_rows[...], wu[...], preferred_element_type=jnp.float32)
        hidden = (gate_act / (1.0 + jnp.exp(-gate_act)) * up_act).astype(jnp.bfloat16)
        y = jnp.dot(hidden, wd[...], preferred_element_type=jnp.float32)
        for c in range(16):
            y_wide[pl.ds(c, count, stride=16), :] = y[:, c * 128:(c + 1) * 128]
        results[first:first + count] = y_wide[...].reshape(count, 16, 128).astype(jnp.bfloat16)

        def start_back(place, carry):
            back(place).start()
            return carry

        lax.fori_loop(max(1, group * GROUP), (group + 1) * GROUP, start_back, 0)
        if group == 0:
            returned[0:SLOTS] = results[0:SLOTS]

    for group in range(128 // GROUP):
        expert_group(group)
    for group in range(128 // GROUP):
        rows = group_rows(group)
        copy(
            results.at[rows], returned.at[rows], back_send, back_recv.at[group], sp, partner
        ).wait_recv()

    def combine(n, carry):
        first = returned[scalars[1, n]].astype(jnp.float32) * weight_ref[0, n]
        second = returned[scalars[2, n]].astype(jnp.float32) * weight_ref[1, n]
        slab_wide[pl.ds(pl.multiple_of(n * 16, 16), 16), :] = first + second
        return carry

    lax.fori_loop(0, 128, combine, 0, unroll=16)
    combined = jnp.concatenate(
        [slab_wide[pl.ds(c, 128, stride=16), :] for c in range(16)], axis=1
    )
    out_ref[...] = (stream[...] + rms_scale(combined, post_ref[...])).astype(jnp.bfloat16)

    for mine, cp in q_copies:
        @pl.when(jnp.logical_not(mine))
        def _():
            cp.wait_send()

    @pl.when(owner)
    def _():
        gate_cp.wait_send()
        own_cp.wait_send()

    def drain(k, carry):
        for d in range(2):
            used, cp = kv_out(k, d)

            @pl.when(used)
            def _():
                cp.wait_send()

        @pl.when(source(k) <= top_block)
        def _():
            passed(k).wait_send()

        return carry

    lax.fori_loop(1, 16, drain, 0)
    for slot in range(2):
        for t in range(8):
            @pl.when(jnp.logical_not((blocks[slot] == sp) & (tp == t)))
            def _():
                o_copy(slot, t).wait_send()
    everything = pl.ds(SLOTS, 127 * SLOTS)
    copy(outgoing.at[everything], arrived_rows.at[everything], go_send, go_recv.at[0], sp, partner).wait_send()
    copy(results.at[everything], returned.at[everything], back_send, back_recv.at[0], sp, partner).wait_send()


def local(
    queries,
    key_rows,
    value_rows,
    cum_gate,
    residual,
    out_weight,
    gain_mix,
    gain_pre,
    gain_post,
    route_ids,
    route_weight,
    w_gate,
    w_up,
    w_down,
):
    tok = queries.shape[0]
    dma = pltpu.SemaphoreType.DMA
    vmem, smem, anywhere = (
        pl.BlockSpec(memory_space=space) for space in (pltpu.VMEM, pltpu.SMEM, pl.ANY)
    )
    bf16, f32 = jnp.bfloat16, jnp.float32
    rows = GROUP * SLOTS
    return pl.pallas_call(
        layer_kernel,
        out_shape=jax.ShapeDtypeStruct((128, 2048), bf16),
        in_specs=[vmem] * 9 + [smem] + [anywhere] * 4,
        out_specs=vmem,
        scratch_shapes=[
            pltpu.VMEM((2, tok // 2, 128), bf16),
            pltpu.VMEM((2, tok, 128), bf16),
            pltpu.VMEM((8, 128 * SLOTS), jnp.int32),
            pltpu.SMEM((8, 128 * SLOTS), jnp.int32),
            pltpu.VMEM((2, tok // 2, 128), bf16),
            pltpu.VMEM((2, tok, 256), bf16),
            pltpu.VMEM((16, tok, 128), jnp.bfloat16),
            pltpu.VMEM((16, tok, 128), jnp.bfloat16),
            pltpu.VMEM((tok, 256), jnp.bfloat16),
            pltpu.VMEM((4, TILE, tok), jnp.float32),
            pltpu.VMEM((tok, 128), bf16),
            pltpu.VMEM((2, 16 * tok), f32),
            pltpu.VMEM((2, tok, 128), f32),
            pltpu.VMEM((2, tok, 128), f32),
            pltpu.VMEM((2, 8, 64, 128), bf16),
            pltpu.VMEM((16, 64, 128), bf16),
            pltpu.VMEM((128, 1024), bf16),
            pltpu.VMEM((1024, 2048), bf16),
            pltpu.VMEM((2048, 512), bf16),
            pltpu.VMEM((2048, 512), bf16),
            pltpu.VMEM((512, 2048), bf16),
            pltpu.VMEM((2048, 128), f32),
            pltpu.VMEM((128, 16, 128), bf16),
            pltpu.VMEM((128, 2048), f32),
            pltpu.VMEM((128 * SLOTS, 16, 128), bf16),
            pltpu.VMEM((128 * SLOTS, 16, 128), bf16),
            pltpu.VMEM((128 * SLOTS, 16, 128), bf16),
            pltpu.VMEM((128 * SLOTS, 16, 128), bf16),
            pltpu.VMEM((rows * 16, 128), f32),
            pltpu.VMEM((rows, 2048), bf16),
            pltpu.VMEM((rows * 16, 128), f32),
            dma((16, 2)), dma((16,)), dma((16,)), dma((16,)), dma((2,)), dma((2,)), dma, dma,
            dma((2, 8)), dma((16,)),
            dma, dma((4,)), dma, dma((128 // GROUP,)), dma, dma((128 // GROUP,)),
        ],
        compiler_params=pltpu.CompilerParams(collective_id=0, has_side_effects=True, vmem_limit_bytes=60 * 1024 * 1024),
        name="layer",
    )(
        queries, key_rows, value_rows, cum_gate, route_ids.T, residual, gain_mix.reshape(1, -1),
        gain_pre.reshape(1, -1), gain_post.reshape(1, -1), route_weight.T,
        out_weight, w_gate[0], w_up[0], w_down[0],
    )


def solution(mesh):
    return jax.shard_map(
        local,
        mesh=mesh,
        in_specs=(
            P("sp", "tp"),
            P("sp", "tp"),
            P("sp", "tp"),
            P("tp", None),
            P(("sp", "tp"), None),
            P(),
            P(),
            P(),
            P(),
            P(("sp", "tp"), None),
            P(("sp", "tp"), None),
            P(("sp", "tp"), None, None),
            P(("sp", "tp"), None, None),
            P(("sp", "tp"), None, None),
        ),
        out_specs=P(("sp", "tp"), None),
        check_vma=False,
    )
```
